32 devices in a mesh: grp: 2 (over x), sp: 4 (over y, core), tp: 4 (over z).
Axes of the slice: x: 2, y: 2, z: 4, core: 2. Of those that a mesh axis runs over, the one named last changes fastest.
Arguments:
- layer_input: bfloat16 [8, 1024, 2048], P(('grp', 'tp'), 'sp'), parts along dimension 0, may hold values from -6 to 6
- norm_gain: bfloat16 [2048], replicated, may hold values from 0.099609375 to 1.8984375
- key_weight: bfloat16 [2048, 1024], replicated, may hold values from -0.125 to 0.125
- value_weight: bfloat16 [2048, 1024], replicated, may hold values from -0.125 to 0.125
- input_gate_weight: bfloat16 [2048, 8], replicated, may hold values from -0.125 to 0.125
- forget_gate_weight: bfloat16 [2048, 8], replicated, may hold values from -0.125 to 0.125
- conv_weight: float32 [4, 1024], replicated, may hold values from -3 to 3
- input_shift: float32 [8, 8, 1024], P(('grp', 'sp'), 'tp'), parts along dimension 0, may hold values from -4 to 302
- forget_shift: float32 [8, 8, 1024], P(('grp', 'sp'), 'tp'), parts along dimension 0, may hold values from 0 to 10.1
- new_query: bfloat16 [8, 8, 128], P(('grp', 'sp'), 'tp'), parts along dimension 0, may hold values from 0.1 to 2
- new_key: bfloat16 [8, 8, 128], P(('grp', 'sp'), 'tp'), parts along dimension 0, may hold values from -6 to 6
- new_value: bfloat16 [8, 8, 128], P(('grp', 'sp'), 'tp'), parts along dimension 0, may hold values from -6 to 6
- new_input: float32 [8, 8], P(('grp', 'sp'), 'tp'), parts along dimension 0, may hold values from 2 to 6
- new_forget: float32 [8, 8], P(('grp', 'sp'), 'tp'), parts along dimension 0, may hold values from -1 to 3
Outputs:
- key_cache: bfloat16 [8, 8, 1024, 128], P(('grp', 'sp'), 'tp'), parts along dimension 0
- value_cache: bfloat16 [8, 8, 1024, 128], P(('grp', 'sp'), 'tp'), parts along dimension 0
- weight_cache: float32 [8, 8, 1024], P(('grp', 'sp'), 'tp'), parts along dimension 0
- first_read: bfloat16 [8, 8, 128], P(('grp', 'sp'), 'tp'), parts along dimension 0
The draws below stay inside these ranges and needn't reach their ends.
There are 2 independent parts, one for each index of `grp`. The reference program is written for one: setup_inputs(seed, part) draws one part's arguments, and reference() takes and returns one part's arrays. A program takes and returns all parts, laid end to end along the dimension named above; an argument that names none is the same for every part. Nothing has to cross between parts.
All inputs are finite; a program needn't handle non-finite values.
Results may differ from the reference program's by a relative error of at most 0.012.
Values may be sent and summed in bfloat16 or wider, within the bound.
A program may use at most 64 MiB of HBM per device.

```python
import jax
import jax.numpy as jnp
from jax import lax

D = 2048
HEADS = 8
DK = 128
CONV = 4
POS_DEV = 256
SEQS = 4
LENGTH = 1024


def draw_input_shift(key, part):
    subkeys = jax.random.split(key, 1)
    return jnp.clip(jax.random.normal(subkeys[0], (SEQS, HEADS, LENGTH), jnp.float32), -4.0, 4.0)


def draw_forget_shift(key, part):
    subkeys = jax.random.split(key, 5)
    slow_share = 0.5
    slower = jax.random.uniform(subkeys[0], (SEQS, HEADS, 1), jnp.float32) < slow_share
    slow_level = jnp.log(jnp.float32(LENGTH))
    fast_level = jax.random.uniform(subkeys[1], (SEQS, HEADS, 1), jnp.float32, 3.4, 4.6)
    block_list = LENGTH // POS_DEV
    factor = jax.random.uniform(subkeys[2], (SEQS, HEADS, block_list, 1), jnp.float32, -0.7, 0.7)
    factor = jnp.broadcast_to(factor, (SEQS, HEADS, block_list, POS_DEV)).reshape(SEQS, HEADS, LENGTH)
    level_values = jnp.where(slower, slow_level, fast_level) + factor
    targets = jax.random.randint(subkeys[3], (SEQS, HEADS, 4), 0, LENGTH)
    level_heights = jax.random.uniform(subkeys[4], (SEQS, HEADS, 4), jnp.float32, 0.0, 1.4)
    places = jnp.arange(LENGTH)
    match_hits = places[None, None, None, :] == targets[:, :, :, None]
    surge_counts = jnp.any(match_hits, axis=2)
    surge_level = jnp.max(jnp.where(match_hits, level_heights[:, :, :, None], -1.0), axis=2)
    return jnp.where(surge_counts, surge_level, level_values)


def draw_new_query(key, part):
    subkeys = jax.random.split(jax.random.fold_in(key, 17), 2)
    drawn = 1.0 + 0.5 * jax.random.normal(subkeys[1], (SEQS, HEADS, DK), jnp.float32)
    return jnp.clip(drawn, 0.1, 2.0).astype(jnp.bfloat16)


def shard_levels(own_key, extent, cuts, least, high):
    level, own = 1.0, jax.random.fold_in(own_key, 6)
    for axis_at, blocks in cuts:
        heights = jnp.exp(jax.random.uniform(jax.random.fold_in(own, axis_at), (blocks,), jnp.float32, least / len(cuts), high / len(cuts)))
        level = level * jnp.repeat(heights, extent[axis_at] // blocks).reshape([-1 if axis == axis_at else 1 for axis in range(len(extent))])
    return level


def bell_draw(own_key, extent, deviation, bound, pieces=(), held_as=jnp.bfloat16):
    values = jax.random.normal(own_key, extent, jnp.float32) * deviation
    if len(pieces) > 0:
        values = shard_levels(own_key, extent, pieces, -0.22, 0.18) * values
    return jnp.clip(values, min=-bound, max=bound).astype(held_as)


def setup_inputs(seed: int = 0, part: int = 0) -> dict:
    key_list = jax.random.split(jax.random.key(seed), 15)
    part_keys = jax.random.split(jax.random.fold_in(key_list[14], part), 15)
    return {
        "layer_input": bell_draw(part_keys[0], (SEQS, LENGTH, D), 1.0, 6.0, ((0, 4), (1, 4))),
        "norm_gain": jnp.clip(1.0 + 0.18 * jax.random.normal(key_list[1], (D,), jnp.float32), 0.099609375, 1.8984375).astype(jnp.bfloat16),
        "key_weight": bell_draw(key_list[2], (D, HEADS * DK), D ** -0.5, 0.125),
        "value_weight": bell_draw(key_list[3], (D, HEADS * DK), D ** -0.5, 0.125),
        "input_gate_weight": bell_draw(key_list[4], (D, HEADS), D ** -0.5, 0.125),
        "forget_gate_weight": bell_draw(key_list[5], (D, HEADS), D ** -0.5, 0.125),
        "conv_weight": bell_draw(key_list[6], (CONV, HEADS * DK), 0.5, 3.0, (), jnp.float32),
        "input_shift": draw_input_shift(jax.random.fold_in(jax.random.fold_in(key_list[14], part), 71), part),
        "forget_shift": draw_forget_shift(jax.random.fold_in(jax.random.fold_in(key_list[14], part), 71), part),
        "new_query": draw_new_query(jax.random.fold_in(jax.random.fold_in(key_list[14], part), 71), part),
        "new_key": bell_draw(part_keys[10], (SEQS, HEADS, DK), 1.0, 6.0, ((0, 4), (1, 4))),
        "new_value": bell_draw(part_keys[11], (SEQS, HEADS, DK), 1.0, 6.0, ((0, 4), (1, 4))),
        "new_input": jnp.clip(2.0 + 4.0 * jax.random.uniform(part_keys[12], (SEQS, HEADS), jnp.float32) ** shard_levels(part_keys[12], (SEQS, HEADS), ((0, 4), (1, 4)), -0.2, 0.2), 2.0, 6.0),
        "new_forget": jnp.clip(-1.0 + 4.0 * jax.random.uniform(part_keys[13], (SEQS, HEADS), jnp.float32) ** shard_levels(part_keys[13], (SEQS, HEADS), ((0, 4), (1, 4)), -0.2, 0.2), -1.0, 3.0),
    }


epsilon = 1e-06

def one_sequence(token_rows, norm_gain, key_weight, value_weight, input_gate_weight, forget_gate_weight, conv_weight):
    widened = token_rows.astype(jnp.float32)
    normed = (widened * lax.rsqrt(lax.optimization_barrier(jnp.mean(widened * widened, axis=-1, keepdims=True)) + epsilon) * norm_gain.astype(jnp.float32)).astype(jnp.bfloat16)
    key_linear = jnp.dot(normed, key_weight, preferred_element_type=jnp.float32).astype(jnp.bfloat16)
    values = jnp.dot(normed, value_weight, preferred_element_type=jnp.float32).astype(jnp.bfloat16)
    input_linear = jnp.dot(normed, input_gate_weight, preferred_element_type=jnp.float32).astype(jnp.bfloat16)
    forget_linear = jnp.dot(normed, forget_gate_weight, preferred_element_type=jnp.float32).astype(jnp.bfloat16)
    padded = jnp.pad(key_linear.astype(jnp.float32), ((CONV - 1, 0), (0, 0)))
    summed = padded[0:LENGTH] * conv_weight[0]
    for offset in range(1, CONV):
        summed = summed + padded[offset:offset + LENGTH] * conv_weight[offset]
    keys = jax.nn.silu(summed).astype(jnp.bfloat16)
    keys = keys.reshape(LENGTH, HEADS, DK).transpose(1, 0, 2)
    values = values.reshape(LENGTH, HEADS, DK).transpose(1, 0, 2)
    return (keys, values, input_linear.T, forget_linear.T)

def read_cache(keys, values, input_linear, forget_linear, input_shift, forget_shift, new_query, new_key, new_value, new_input, new_forget):
    scaling = DK ** (-0.5)
    log_forget = jax.nn.log_sigmoid(forget_linear.astype(jnp.float32) + forget_shift)
    suffix = lax.cumsum(log_forget, axis=2, reverse=True) - log_forget
    new_decay = jax.nn.log_sigmoid(new_forget)
    log_weight = input_linear.astype(jnp.float32) + input_shift + suffix + new_decay[:, :, None]
    largest = jnp.maximum(lax.optimization_barrier(jnp.max(log_weight, axis=2)), new_input)
    weight_cache = jnp.exp(log_weight - largest[:, :, None])
    new_weight = jnp.exp(new_input - largest)
    matched = jnp.einsum('bhlk,bhk->bhl', keys.astype(jnp.float32), new_query.astype(jnp.float32))
    scores = (weight_cache * matched * scaling).astype(jnp.bfloat16)
    fresh_match = lax.optimization_barrier(jnp.sum(new_key.astype(jnp.float32) * new_query.astype(jnp.float32), axis=2))
    new_score = (new_weight * fresh_match * scaling).astype(jnp.bfloat16)
    denominator = lax.optimization_barrier(jnp.sum(scores.astype(jnp.float32), axis=2)) + new_score.astype(jnp.float32)
    numerator = jnp.einsum('bhl,bhlk->bhk', scores.astype(jnp.float32), values.astype(jnp.float32))
    numerator = numerator + new_score.astype(jnp.float32)[:, :, None] * new_value.astype(jnp.float32)
    first_read = (numerator / jnp.maximum(jnp.abs(denominator), 1.0)[:, :, None]).astype(jnp.bfloat16)
    return (weight_cache, first_read)

def reference(layer_input, norm_gain, key_weight, value_weight, input_gate_weight, forget_gate_weight, conv_weight, input_shift, forget_shift, new_query, new_key, new_value, new_input, new_forget):

    def project(token_rows):
        return one_sequence(token_rows, norm_gain, key_weight, value_weight, input_gate_weight, forget_gate_weight, conv_weight)
    keys, values, input_linear, forget_linear = lax.map(project, layer_input)
    weight_cache, first_read = read_cache(keys, values, input_linear, forget_linear, input_shift, forget_shift, new_query, new_key, new_value, new_input, new_forget)
    return (keys, values, weight_cache, first_read)
```

```python
import functools

import jax
import jax.numpy as jnp
from jax import lax
from jax.experimental import pallas as pl
from jax.experimental.pallas import tpu as pltpu
from jax.sharding import PartitionSpec as P

MESH = pl.DeviceIdType.MESH
epsilon = 1e-06


def log_sigmoid(x):
    return jnp.minimum(x, 0.0) - jnp.log1p(jnp.exp(-jnp.abs(x)))


def kernel(
    dims,
    x_hbm,
    gain_hbm,
    wi_hbm,
    wf_hbm,
    conv_hbm,
    ishift_hbm,
    fshift_hbm,
    query_hbm,
    nkey_hbm,
    nvalue_hbm,
    ninput_hbm,
    nforget_hbm,
    wk_hbm,
    wv_hbm,
    keys_out,
    values_out,
    weight_out,
    read_out,
    x_ref,
    gain_ref,
    wgate,
    conv_ref,
    ishift_ref,
    fshift_ref,
    query_ref,
    nkey_ref,
    nvalue_ref,
    ninput_ref,
    nforget_ref,
    wbuf,
    scaled,
    normed,
    rs,
    comp,
    gcomp,
    final,
    gfinal,
    ext,
    in_sem,
    w_sem,
    small_sem,
    send_sem,
    f_recv,
):
    n, nsp, ns, nd, pos, heads, hl, dk, taps = dims
    G = 2
    length = nsp * pos
    width = x_ref.shape[2]
    nt = max(1, nd // ns)
    nq = max(1, ns // nd)
    t = lax.axis_index("tp")
    p = lax.axis_index("sp")
    low = 2 * t < n

    first = (p * nd) // ns
    barrier = pltpu.get_barrier_semaphore()
    for m in range(nt):
        for a in range(nsp):
            peer = {"sp": lax.rem(p + a, nsp), "tp": first + m}

            def greet(peer=peer):
                pl.semaphore_signal(barrier, inc=1, device_id=peer, device_id_type=MESH)

            if a:
                greet()
            else:
                pl.when(first + m != t)(greet)
    own = ((t >= first) & (t < first + nt)).astype(jnp.int32)

    def target(k):
        down = jnp.where(k < n - 1 - t, n - 1 - k, n - 2 - k)
        up = jnp.where(k < t, k, k + 1)
        return jnp.where(k == n - 1, t, jnp.where(low, down, up))

    def weight_copy(k, kv):
        columns = pl.ds(pl.multiple_of(target(k) * (hl * dk), dk), hl * dk)
        source = wv_hbm if kv else wk_hbm
        return pltpu.make_async_copy(source.at[:, columns], wbuf.at[k, kv], w_sem.at[k, kv])

    x_copy = pltpu.make_async_copy(x_hbm, x_ref, in_sem.at[0])
    gain_copy = pltpu.make_async_copy(gain_hbm, gain_ref, in_sem.at[1])
    wi_copy = pltpu.make_async_copy(wi_hbm, wgate.at[0:heads], in_sem.at[2])
    wf_copy = pltpu.make_async_copy(wf_hbm, wgate.at[heads : 2 * heads], in_sem.at[3])
    x_copy.start()
    gain_copy.start()
    weight_copy(0, 0).start()
    weight_copy(0, 1).start()
    wi_copy.start()
    wf_copy.start()
    for k in range(1, n):
        for kv in range(2):
            weight_copy(k, kv).start()
    own_columns = pl.ds(pl.multiple_of(t * (hl * dk), dk), hl * dk)
    small = [
        pltpu.make_async_copy(a, b, small_sem.at[at])
        for at, (a, b) in enumerate(
            (
                (conv_hbm.at[:, own_columns], conv_ref),
                (ishift_hbm, ishift_ref),
                (fshift_hbm, fshift_ref),
                (query_hbm, query_ref),
                (nkey_hbm, nkey_ref),
                (nvalue_hbm, nvalue_ref),
                (ninput_hbm, ninput_ref),
                (nforget_hbm, nforget_ref),
            )
        )
    ]
    for copy in small:
        copy.start()

    gain_copy.wait()
    gain = gain_ref[...].astype(jnp.float32).reshape(1, -1)
    x_copy.wait()
    step = 32
    for i in range(ns):
        for at in range(0, pos, step):
            wide = x_ref[i, at : at + step, :].astype(jnp.float32)
            scaled[i, at : at + step, :] = (wide * gain).astype(jnp.bfloat16)
            mean = jnp.mean(wide * wide, axis=-1, keepdims=True)
            rs[i, at : at + step, :] = jnp.broadcast_to(lax.rsqrt(mean + epsilon), (step, dk))

    def s_source(k, i, c):
        return gcomp.at[i] if c == G else comp.at[k, i, c]

    def f_target(d, at, c):
        if c == G:
            return gfinal.at[d, at]
        window = pl.ds(pl.multiple_of(at * pos, pos), pos)
        return (values_out if c else final).at[d, :, window, :]

    def send(k, i, c, begin):
        s = t * ns + i
        q = s // nd
        d = lax.rem(s, nd)
        source = s_source(k, i, c)
        remote = pltpu.make_async_remote_copy(
            src_ref=source,
            dst_ref=f_target(d, p, c),
            send_sem=send_sem.at[k, i, c],
            recv_sem=f_recv.at[d, p, c],
            device_id={"sp": q, "tp": target(k)},
            device_id_type=MESH,
        )
        away = (k < n - 1) | (q != p)

        @pl.when(away)
        def _():
            if begin:
                remote.start()
            else:
                remote.wait_send()

        if begin:

            @pl.when(jnp.logical_not(away))
            def _():
                pltpu.make_async_copy(source, f_target(d, p, c), f_recv.at[d, p, c]).start()

    def gates():
        wi_copy.wait()
        wf_copy.wait()
        for i in range(ns):

            @pl.loop(0, pos // step)
            def _(at):
                window = pl.ds(pl.multiple_of(at * step, step), step)
                wide = x_ref[i, window, :].astype(jnp.float32)
                normed[i, window, :] = (wide * rs[i, window, 0:1] * gain).astype(jnp.bfloat16)

            g = lax.dot_general(
                normed[i], wgate[...], (((1,), (1,)), ((), ())), preferred_element_type=jnp.float32
            )
            gcomp[i] = g.T.astype(jnp.bfloat16)

    @pl.loop(0, n)
    def _(k):
        for kv in range(2):
            weight_copy(k, kv).wait()
            for i in range(ns):
                y = jnp.dot(scaled[i], wbuf[k, kv], preferred_element_type=jnp.float32)
                for h in range(hl):
                    comp[k, i, kv, h] = (y[:, h * dk : (h + 1) * dk] * rs[i]).astype(jnp.bfloat16)
            if kv == 0:

                @pl.when(k == 0)
                def _():
                    pl.semaphore_wait(barrier, nq * n - own)

            for i in range(ns):
                send(k, i, kv, True)

        @pl.when(k == 0)
        def _():
            gates()
            for to in range(n):
                for i in range(ns):
                    send(to, i, G, True)

    def arrived(d, at, c):
        place = f_target(d, at, c)
        pltpu.make_async_copy(place, place, f_recv.at[d, at, c]).wait()

    scaling = dk ** (-0.5)
    lane = lax.broadcasted_iota(jnp.int32, (8, length), 1)
    row = lax.broadcasted_iota(jnp.int32, (2 * heads, pos), 0)
    weights, fresh, scores = {}, {}, {}
    for copy in small:
        copy.wait()

    for d in range(nd):
        for at in range(nsp):
            arrived(d, at, G)
        for h in range(hl):

            def gate(base):
                pieces = [
                    jnp.sum(
                        jnp.where(row == base + t * hl + h, gfinal[d, at].astype(jnp.float32), 0.0),
                        axis=0,
                        keepdims=True,
                    )
                    for at in range(nsp)
                ]
                return jnp.concatenate(pieces, axis=1)

            log_forget = log_sigmoid(gate(heads) + fshift_ref[d, h : h + 1, :])
            suffix = pltpu.roll(jnp.broadcast_to(log_forget, (8, length)), length - 1, 1)
            suffix = jnp.where(lane < length - 1, suffix, 0.0)
            hop = 1
            while hop < length:
                moved = pltpu.roll(suffix, length - hop, 1)
                suffix = suffix + jnp.where(lane < length - hop, moved, 0.0)
                hop *= 2
            new_input = ninput_ref[d : d + 1, h : h + 1]
            decay = log_sigmoid(nforget_ref[d : d + 1, h : h + 1])
            log_weight = gate(0) + ishift_ref[d, h : h + 1, :] + suffix + decay
            largest = jnp.maximum(jnp.max(log_weight, axis=1, keepdims=True), new_input)
            weight = jnp.exp(log_weight - largest)
            weight_out[d, h : h + 1, :] = weight[0:1]
            query = query_ref[d, h : h + 1, :].astype(jnp.float32)
            match = jnp.sum(
                nkey_ref[d, h : h + 1, :].astype(jnp.float32) * query, axis=1, keepdims=True
            )
            score = jnp.exp(new_input - largest) * match * scaling
            fresh[d, h] = score.astype(jnp.bfloat16).astype(jnp.float32)
            weights[d, h] = weight

    for d in range(nd):
        ext[:, 0:8, :] = jnp.zeros((hl, 8, dk), jnp.float32)
        for at in range(nsp):
            arrived(d, at, 0)
            for h in range(hl):
                ext[h, 8 + at * pos : 8 + (at + 1) * pos, :] = final[
                    d, h, at * pos : (at + 1) * pos, :
                ].astype(jnp.float32)
                tap = conv_ref[:, h * dk : (h + 1) * dk]
                summed = None
                for o in range(taps):
                    start = 8 - (taps - 1) + o + at * pos
                    term = ext[h, start : start + pos, :] * tap[o : o + 1, :]
                    summed = term if summed is None else summed + term
                keys_out[d, h, at * pos : (at + 1) * pos, :] = jax.nn.silu(summed).astype(
                    jnp.bfloat16
                )
        for h in range(hl):
            query = jnp.broadcast_to(query_ref[d, h : h + 1, :], (8, dk))
            matched = lax.dot_general(
                query, keys_out[d, h], (((1,), (1,)), ((), ())), preferred_element_type=jnp.float32
            )
            scores[d, h] = (weights[d, h] * matched * scaling).astype(jnp.bfloat16)

    for d in range(nd):
        for at in range(nsp):
            arrived(d, at, 1)
        for h in range(hl):
            score = scores[d, h]
            denominator = jnp.sum(score.astype(jnp.float32), axis=1, keepdims=True) + fresh[d, h]
            numerator = jnp.dot(score, values_out[d, h], preferred_element_type=jnp.float32)
            numerator = numerator + fresh[d, h] * nvalue_ref[d, h : h + 1, :].astype(jnp.float32)
            result = numerator / jnp.maximum(jnp.abs(denominator), 1.0)
            read_out[d, h : h + 1, :] = result[0:1].astype(jnp.bfloat16)

    for k in range(n):
        for i in range(ns):
            for c in range(G + 1):
                send(k, i, c, False)


def write_out(*refs):
    count = (len(refs) - 1) // 2
    sem = refs[-1]
    copies = [
        pltpu.make_async_copy(refs[i], refs[count + i], sem.at[i]) for i in range(count)
    ]
    for copy in copies:
        copy.start()
    for copy in copies:
        copy.wait()


def shards(
    n,
    nsp,
    layer_input,
    norm_gain,
    key_weight,
    value_weight,
    input_gate_weight,
    forget_gate_weight,
    conv_weight,
    input_shift,
    forget_shift,
    new_query,
    new_key,
    new_value,
    new_input,
    new_forget,
):
    ns, pos, width = layer_input.shape
    nd, hl, length = input_shift.shape
    dk = new_query.shape[2]
    heads = input_gate_weight.shape[1]
    taps = conv_weight.shape[0]
    dims = (n, nsp, ns, nd, pos, heads, hl, dk, taps)
    bf16, f32 = jnp.bfloat16, jnp.float32
    vmem = pl.BlockSpec(memory_space=pltpu.VMEM)
    hbm = pl.BlockSpec(memory_space=pltpu.HBM)
    dma = pltpu.SemaphoreType.DMA
    out_shape = (
        jax.ShapeDtypeStruct((nd, hl, length, dk), bf16),
        jax.ShapeDtypeStruct((nd, hl, length, dk), bf16),
        jax.ShapeDtypeStruct((nd, hl, length), f32),
        jax.ShapeDtypeStruct((nd, hl, dk), bf16),
    )
    held = pl.pallas_call(
        functools.partial(kernel, dims),
        out_shape=tuple(pltpu.VMEM(o.shape, o.dtype) for o in out_shape),
        in_specs=[hbm] * 14,
        out_specs=(vmem,) * 4,
        scratch_shapes=[
            pltpu.VMEM((ns, pos, width), bf16),
            pltpu.VMEM((width,), bf16),
            pltpu.VMEM((2 * heads, width), bf16),
            pltpu.VMEM((taps, hl * dk), f32),
            pltpu.VMEM((nd, hl, length), f32),
            pltpu.VMEM((nd, hl, length), f32),
            pltpu.VMEM((nd, hl, dk), bf16),
            pltpu.VMEM((nd, hl, dk), bf16),
            pltpu.VMEM((nd, hl, dk), bf16),
            pltpu.VMEM((nd, hl), f32),
            pltpu.VMEM((nd, hl), f32),
            pltpu.VMEM((n, 2, width, hl * dk), bf16),
            pltpu.VMEM((ns, pos, width), bf16),
            pltpu.VMEM((ns, pos, width), bf16),
            pltpu.VMEM((ns, pos, dk), f32),
            pltpu.VMEM((n, ns, 2, hl, pos, dk), bf16),
            pltpu.VMEM((ns, 2 * heads, pos), bf16),
            pltpu.VMEM((nd, hl, length, dk), bf16),
            pltpu.VMEM((nd, nsp, 2 * heads, pos), bf16),
            pltpu.VMEM((hl, 8 + length, dk), f32),
            dma((4,)),
            dma((n, 2)),
            dma((8,)),
            dma((n, ns, 3)),
            dma((nd, nsp, 3)),
        ],
        compiler_params=pltpu.CompilerParams(
            collective_id=0, has_side_effects=True, vmem_limit_bytes=60 * 1024 * 1024
        ),
    )(
        layer_input,
        norm_gain,
        input_gate_weight.T,
        forget_gate_weight.T,
        conv_weight,
        input_shift,
        forget_shift,
        new_query,
        new_key,
        new_value,
        new_input,
        new_forget,
        key_weight,
        value_weight,
    )
    return pl.pallas_call(
        write_out,
        out_shape=out_shape,
        in_specs=[vmem] * len(out_shape),
        out_specs=(hbm,) * len(out_shape),
        scratch_shapes=[dma((len(out_shape),))],
        compiler_params=pltpu.CompilerParams(vmem_limit_bytes=8 * 1024 * 1024),
    )(*held)


def solution(mesh):
    in_specs = (
        P(("grp", "tp"), "sp", None),
        P(),
        P(),
        P(),
        P(),
        P(),
        P(),
        P(("grp", "sp"), "tp", None),
        P(("grp", "sp"), "tp", None),
        P(("grp", "sp"), "tp", None),
        P(("grp", "sp"), "tp", None),
        P(("grp", "sp"), "tp", None),
        P(("grp", "sp"), "tp"),
        P(("grp", "sp"), "tp"),
    )
    out_specs = (
        P(("grp", "sp"), "tp", None, None),
        P(("grp", "sp"), "tp", None, None),
        P(("grp", "sp"), "tp", None),
        P(("grp", "sp"), "tp", None),
    )
    body = functools.partial(shards, mesh.shape["tp"], mesh.shape["sp"])
    return jax.shard_map(body, mesh=mesh, in_specs=in_specs, out_specs=out_specs, check_vma=False)
```

```python
import functools

import jax
import jax.numpy as jnp
from jax import lax
from jax.experimental import pallas as pl
from jax.experimental.pallas import tpu as pltpu
from jax.sharding import PartitionSpec as P

MESH = pl.DeviceIdType.MESH
epsilon = 1e-06
HALVES = 2


def log_sigmoid(x):
    return jnp.minimum(x, 0.0) - jnp.log1p(jnp.exp(-jnp.abs(x)))


def kernel(
    dims,
    x_hbm,
    gain_hbm,
    wi_hbm,
    wf_hbm,
    conv_hbm,
    ishift_hbm,
    fshift_hbm,
    query_hbm,
    nkey_hbm,
    nvalue_hbm,
    ninput_hbm,
    nforget_hbm,
    wk_hbm,
    wv_hbm,
    keys_out,
    values_out,
    weight_out,
    read_out,
    x_ref,
    gain_ref,
    wgate,
    conv_ref,
    shifts,
    fresh_rows,
    fresh_gates,
    wbuf,
    scaled,
    normed,
    rs,
    comp,
    gcomp,
    final,
    gfinal,
    ext,
    x_sem,
    in_sem,
    w_sem,
    send_sem,
    f_recv,
    ready,
):
    n, nsp, ns, nd, pos, heads, hl, dk, taps = dims
    G = 2
    length = nsp * pos
    width = x_ref.shape[2]
    nt = max(1, nd // ns)
    nq = max(1, ns // nd)
    t = lax.axis_index("tp")
    p = lax.axis_index("sp")
    low = 2 * t < n

    first = (p * nd) // ns
    late = n >= 4
    far = t == n - 1 if late else False
    barrier = pltpu.get_barrier_semaphore()

    def tell(semaphore, sp, tp):
        pl.semaphore_signal(
            semaphore, inc=1, device_id={"sp": sp, "tp": tp}, device_id_type=MESH
        )

    def greet(only_far):
        for m in range(nt):
            for a in range(nsp):
                to = first + m
                wanted = None if a else to != t
                if only_far:
                    wanted = to == n - 1 if a else (to == n - 1) & (to != t)

                def one(a=a, to=to):
                    tell(barrier, lax.rem(p + a, nsp), to)

                one() if wanted is None else pl.when(wanted)(one)

    own = ((t >= first) & (t < first + nt)).astype(jnp.int32)
    if late:

        @pl.when(far)
        def _():
            greet(True)

        @pl.when(jnp.logical_not(far))
        def _():
            for m in range(nq):
                tell(barrier, (t * ns) // nd + m, n - 1)
            greet(False)

        ends = ((first <= n - 1) & (n - 1 < first + nt)).astype(jnp.int32)
        expected = jnp.where(far, nq * n - own + nsp * (nt - ends), nq * (n - 1) - own)
    else:
        greet(False)
        expected = nq * n - own

    def met():
        pl.semaphore_wait(barrier, expected)
        if late:

            @pl.when(far)
            def _():
                for m in range(nt):
                    for a in range(nsp):

                        @pl.when(first + m != n - 1)
                        def _():
                            tell(ready, lax.rem(p + a, nsp), first + m)

    def target(k):
        down = jnp.where(k < n - 1 - t, n - 1 - k, n - 2 - k)
        if late:
            down = jnp.where(k == 0, n - 2, jnp.where(k == 1, n - 1, down))
        up = jnp.where(k < t, k, k + 1)
        return jnp.where(k == n - 1, t, jnp.where(low, down, up))

    def weight_copy(k, kv):
        columns = pl.ds(pl.multiple_of(target(k) * (hl * dk), dk), hl * dk)
        source = wv_hbm if kv else wk_hbm
        slot = kv if isinstance(k, int) and k == 0 else 1 + k
        return pltpu.make_async_copy(source.at[:, columns], wbuf.at[k, kv], w_sem.at[slot])

    half = pos // HALVES
    x_copies = [
        pltpu.make_async_copy(
            x_hbm.at[:, at * half : (at + 1) * half], x_ref.at[:, at * half : (at + 1) * half], x_sem.at[at]
        )
        for at in range(HALVES)
    ]
    own_columns = pl.ds(pl.multiple_of(t * (hl * dk), dk), hl * dk)
    groups = (
        (gain_ref, ((gain_hbm, gain_ref),)),
        (wgate, ((wi_hbm, wgate.at[0:heads]), (wf_hbm, wgate.at[heads : 2 * heads]))),
        (conv_ref, ((conv_hbm.at[:, own_columns], conv_ref),)),
        (shifts, ((ishift_hbm, shifts.at[0]), (fshift_hbm, shifts.at[1]))),
        (
            fresh_rows,
            ((query_hbm, fresh_rows.at[0]), (nkey_hbm, fresh_rows.at[1]), (nvalue_hbm, fresh_rows.at[2])),
        ),
        (fresh_gates, ((ninput_hbm, fresh_gates.at[0]), (nforget_hbm, fresh_gates.at[1]))),
    )

    def load(g):
        for source, place in groups[g][1]:
            pltpu.make_async_copy(source, place, in_sem.at[g]).start()

    def loaded(g):
        whole = groups[g][0]
        pltpu.make_async_copy(whole, whole, in_sem.at[g]).wait()

    load(0)
    x_copies[0].start()
    weight_copy(0, 0).start()
    for copy in x_copies[1:]:
        copy.start()

    def start_rest():
        weight_copy(0, 1).start()
        load(1)
        for k in range(1, n):
            for kv in range(2):
                weight_copy(k, kv).start()
        for g in range(2, len(groups)):
            load(g)

    loaded(0)
    gain = gain_ref[...].astype(jnp.float32).reshape(1, -1)
    step = 32

    def scale(part):
        x_copies[part].wait()
        for i in range(ns):
            for at in range(part * half, (part + 1) * half, step):
                wide = x_ref[i, at : at + step, :].astype(jnp.float32)
                scaled[i, at : at + step, :] = (wide * gain).astype(jnp.bfloat16)
                mean = jnp.mean(wide * wide, axis=-1, keepdims=True)
                rs[i, at : at + step, :] = jnp.broadcast_to(lax.rsqrt(mean + epsilon), (step, dk))

    def send(k, i, c, part=None):
        s = t * ns + i
        q = s // nd
        d = lax.rem(s, nd)
        to = k if c == G else target(k)
        mine = to == t
        if c == G:
            source, place = gcomp.at[k, i], gfinal.at[d, p]
        else:
            rows = half if part is not None else pos
            lead = half * part if part is not None else 0
            source = comp.at[k, i, c, :, pl.ds(lead, rows), :]
            window = pl.ds(pl.multiple_of(p * pos + lead, rows), rows)
            place = (values_out if c else final).at[d, :, window, :]
        slot = jnp.where(mine, 1, 0)
        remote = pltpu.make_async_remote_copy(
            src_ref=source,
            dst_ref=place,
            send_sem=send_sem.at[slot, c // G],
            recv_sem=f_recv.at[d, c],
            device_id={"sp": q, "tp": to},
            device_id_type=MESH,
        )
        away = jnp.logical_not(mine & (q == p))
        pl.when(away)(lambda: remote.start())

        @pl.when(jnp.logical_not(away))
        def _():
            pltpu.make_async_copy(source, place, f_recv.at[d, c]).start()

    def gates():
        loaded(1)
        for i in range(ns):

            @pl.loop(0, pos // step)
            def _(at):
                window = pl.ds(pl.multiple_of(at * step, step), step)
                wide = x_ref[i, window, :].astype(jnp.float32)
                normed[i, window, :] = (wide * rs[i, window, 0:1] * gain).astype(jnp.bfloat16)

            g = lax.dot_general(
                normed[i], wgate[...], (((1,), (1,)), ((), ())), preferred_element_type=jnp.float32
            )
            g = g.T
            for to in range(n):
                lines = [
                    g[base + to * hl + h : base + to * hl + h + 1, at * 128 : (at + 1) * 128]
                    for base in (0, heads)
                    for h in range(hl)
                    for at in range(pos // 128)
                ]
                gcomp[to, i] = jnp.concatenate(lines, axis=0).astype(jnp.bfloat16)

    def project(k, kv, lead, rows):
        for i in range(ns):
            y = jnp.dot(
                scaled[i, lead : lead + rows], wbuf[k, kv], preferred_element_type=jnp.float32
            )
            for h in range(hl):
                comp[k, i, kv, h, lead : lead + rows] = (
                    y[:, h * dk : (h + 1) * dk] * rs[i, lead : lead + rows]
                ).astype(jnp.bfloat16)

    scale(0)
    weight_copy(0, 0).wait()
    start_rest()
    for part in range(HALVES):
        if part:
            scale(part)
        project(0, 0, part * half, half)
        if part == 0:
            met()
        for i in range(ns):
            send(0, i, 0, part)
    weight_copy(0, 1).wait()
    project(0, 1, 0, pos)
    for i in range(ns):
        send(0, i, 1)
    gates()
    if late:

        @pl.when(jnp.logical_not(far))
        def _():
            pl.semaphore_wait(ready, nq)

    for to in range(n):
        for i in range(ns):
            send(to, i, G)

    @pl.loop(1, n)
    def _(k):
        pltpu.make_async_copy(wbuf.at[k], wbuf.at[k], w_sem.at[1 + k]).wait()
        for kv in range(2):
            project(k, kv, 0, pos)
            for i in range(ns):
                send(k, i, kv)

    def arrived(d, c):
        place = (final.at[d], values_out.at[d], gfinal.at[d])[c]
        pltpu.make_async_copy(place, place, f_recv.at[d, c]).wait()

    scaling = dk ** (-0.5)
    lane = lax.broadcasted_iota(jnp.int32, (8, length), 1)
    weights, fresh, scores = {}, {}, {}
    for g in range(2, len(groups)):
        loaded(g)

    for d in range(nd):
        arrived(d, G)
        for h in range(hl):

            def gate(which):
                lead = (which * hl + h) * (pos // 128)
                return jnp.concatenate(
                    [
                        gfinal[d, at].astype(jnp.float32)[lead + q : lead + q + 1]
                        for at in range(nsp)
                        for q in range(pos // 128)
                    ],
                    axis=1,
                )

            log_forget = log_sigmoid(gate(1) + shifts[1, d, h : h + 1, :])
            suffix = pltpu.roll(jnp.broadcast_to(log_forget, (8, length)), length - 1, 1)
            suffix = jnp.where(lane < length - 1, suffix, 0.0)
            hop = 1
            while hop < length:
                moved = pltpu.roll(suffix, length - hop, 1)
                suffix = suffix + jnp.where(lane < length - hop, moved, 0.0)
                hop *= 2
            new_input = fresh_gates[0, d : d + 1, h : h + 1]
            decay = log_sigmoid(fresh_gates[1, d : d + 1, h : h + 1])
            log_weight = gate(0) + shifts[0, d, h : h + 1, :] + suffix + decay
            largest = jnp.maximum(jnp.max(log_weight, axis=1, keepdims=True), new_input)
            weight = jnp.exp(log_weight - largest)
            weight_out[d, h : h + 1, :] = weight[0:1]
            query = fresh_rows[0, d, h : h + 1, :].astype(jnp.float32)
            match = jnp.sum(
                fresh_rows[1, d, h : h + 1, :].astype(jnp.float32) * query, axis=1, keepdims=True
            )
            score = jnp.exp(new_input - largest) * match * scaling
            fresh[d, h] = score.astype(jnp.bfloat16).astype(jnp.float32)
            weights[d, h] = weight

    for d in range(nd):
        ext[:, 0:8, :] = jnp.zeros((hl, 8, dk), jnp.float32)
        arrived(d, 0)
        for at in range(nsp):
            for h in range(hl):
                ext[h, 8 + at * pos : 8 + (at + 1) * pos, :] = final[
                    d, h, at * pos : (at + 1) * pos, :
                ].astype(jnp.float32)
                tap = conv_ref[:, h * dk : (h + 1) * dk]
                summed = None
                for o in range(taps):
                    start = 8 - (taps - 1) + o + at * pos
                    term = ext[h, start : start + pos, :] * tap[o : o + 1, :]
                    summed = term if summed is None else summed + term
                keys_out[d, h, at * pos : (at + 1) * pos, :] = jax.nn.silu(summed).astype(
                    jnp.bfloat16
                )
        for h in range(hl):
            query = jnp.broadcast_to(fresh_rows[0, d, h : h + 1, :], (8, dk))
            matched = lax.dot_general(
                query, keys_out[d, h], (((1,), (1,)), ((), ())), preferred_element_type=jnp.float32
            )
            scores[d, h] = (weights[d, h] * matched * scaling).astype(jnp.bfloat16)

    for d in range(nd):
        arrived(d, 1)
        for h in range(hl):
            score = scores[d, h]
            denominator = jnp.sum(score.astype(jnp.float32), axis=1, keepdims=True) + fresh[d, h]
            numerator = jnp.dot(score, values_out[d, h], preferred_element_type=jnp.float32)
            numerator = numerator + fresh[d, h] * fresh_rows[2, d, h : h + 1, :].astype(jnp.float32)
            result = numerator / jnp.maximum(jnp.abs(denominator), 1.0)
            read_out[d, h : h + 1, :] = result[0:1].astype(jnp.bfloat16)

    def sent(place, slot, c):
        pltpu.make_async_copy(place, place, send_sem.at[slot, c]).wait()

    if n > 1:
        sent(comp.at[0 : n - 1], 0, 0)
        sent(gcomp.at[0 : n - 1], 0, 1)
    kept = sum(((t * ns + i) // nd == p).astype(jnp.int32) for i in range(ns))
    for count in range(ns):

        @pl.when(kept == count)
        def _():
            sent(comp.at[n - 1, 0 : ns - count], 1, 0)
            sent(gcomp.at[n - 1, 0 : ns - count], 1, 1)


def write_out(*refs):
    count = (len(refs) - 1) // 2
    sem = refs[-1]
    copies = [
        pltpu.make_async_copy(refs[i], refs[count + i], sem.at[i]) for i in range(count)
    ]
    for copy in copies:
        copy.start()
    for copy in copies:
        copy.wait()


def shards(
    n,
    nsp,
    layer_input,
    norm_gain,
    key_weight,
    value_weight,
    input_gate_weight,
    forget_gate_weight,
    conv_weight,
    input_shift,
    forget_shift,
    new_query,
    new_key,
    new_value,
    new_input,
    new_forget,
):
    ns, pos, width = layer_input.shape
    nd, hl, length = input_shift.shape
    dk = new_query.shape[2]
    heads = input_gate_weight.shape[1]
    taps = conv_weight.shape[0]
    dims = (n, nsp, ns, nd, pos, heads, hl, dk, taps)
    bf16, f32 = jnp.bfloat16, jnp.float32
    vmem = pl.BlockSpec(memory_space=pltpu.VMEM)
    hbm = pl.BlockSpec(memory_space=pltpu.HBM)
    dma = pltpu.SemaphoreType.DMA
    out_shape = (
        jax.ShapeDtypeStruct((nd, hl, length, dk), bf16),
        jax.ShapeDtypeStruct((nd, hl, length, dk), bf16),
        jax.ShapeDtypeStruct((nd, hl, length), f32),
        jax.ShapeDtypeStruct((nd, hl, dk), bf16),
    )
    held = pl.pallas_call(
        functools.partial(kernel, dims),
        out_shape=tuple(pltpu.VMEM(o.shape, o.dtype) for o in out_shape),
        in_specs=[hbm] * 14,
        out_specs=(vmem,) * 4,
        scratch_shapes=[
            pltpu.VMEM((ns, pos, width), bf16),
            pltpu.VMEM((width,), bf16),
            pltpu.VMEM((2 * heads, width), bf16),
            pltpu.VMEM((taps, hl * dk), f32),
            pltpu.VMEM((2, nd, hl, length), f32),
            pltpu.VMEM((3, nd, hl, dk), bf16),
            pltpu.VMEM((2, nd, hl), f32),
            pltpu.VMEM((n, 2, width, hl * dk), bf16),
            pltpu.VMEM((ns, pos, width), bf16),
            pltpu.VMEM((ns, pos, width), bf16),
            pltpu.VMEM((ns, pos, dk), f32),
            pltpu.VMEM((n, ns, 2, hl, pos, dk), bf16),
            pltpu.VMEM((n, ns, 2 * hl * pos // 128, 128), bf16),
            pltpu.VMEM((nd, hl, length, dk), bf16),
            pltpu.VMEM((nd, nsp, 2 * hl * pos // 128, 128), bf16),
            pltpu.VMEM((hl, 8 + length, dk), f32),
            dma((HALVES,)),
            dma((6,)),
            dma((n + 1,)),
            dma((2, 2)),
            dma((nd, 3)),
            pltpu.SemaphoreType.REGULAR,
        ],
        compiler_params=pltpu.CompilerParams(
            collective_id=0, has_side_effects=True, vmem_limit_bytes=60 * 1024 * 1024
        ),
    )(
        layer_input,
        norm_gain,
        input_gate_weight.T,
        forget_gate_weight.T,
        conv_weight,
        input_shift,
        forget_shift,
        new_query,
        new_key,
        new_value,
        new_input,
        new_forget,
        key_weight,
        value_weight,
    )
    return pl.pallas_call(
        write_out,
        out_shape=out_shape,
        in_specs=[vmem] * len(out_shape),
        out_specs=(hbm,) * len(out_shape),
        scratch_shapes=[dma((len(out_shape),))],
        compiler_params=pltpu.CompilerParams(vmem_limit_bytes=8 * 1024 * 1024),
    )(*held)


def solution(mesh):
    in_specs = (
        P(("grp", "tp"), "sp", None),
        P(),
        P(),
        P(),
        P(),
        P(),
        P(),
        P(("grp", "sp"), "tp", None),
        P(("grp", "sp"), "tp", None),
        P(("grp", "sp"), "tp", None),
        P(("grp", "sp"), "tp", None),
        P(("grp", "sp"), "tp", None),
        P(("grp", "sp"), "tp"),
        P(("grp", "sp"), "tp"),
    )
    out_specs = (
        P(("grp", "sp"), "tp", None, None),
        P(("grp", "sp"), "tp", None, None),
        P(("grp", "sp"), "tp", None),
        P(("grp", "sp"), "tp", None),
    )
    body = functools.partial(shards, mesh.shape["tp"], mesh.shape["sp"])
    return jax.shard_map(body, mesh=mesh, in_specs=in_specs, out_specs=out_specs, check_vma=False)
```

```python
import functools

import jax
import jax.numpy as jnp
from jax import lax
from jax.experimental import pallas as pl
from jax.experimental.pallas import tpu as pltpu
from jax.sharding import PartitionSpec as P

MESH = pl.DeviceIdType.MESH
epsilon = 1e-06
EARLY = 2


def log_sigmoid(x):
    return jnp.minimum(x, 0.0) - jnp.log1p(jnp.exp(-jnp.abs(x)))


def kernel(
    dims,
    x_hbm,
    gain_hbm,
    wi_hbm,
    wf_hbm,
    conv_hbm,
    ishift_hbm,
    fshift_hbm,
    query_hbm,
    nkey_hbm,
    nvalue_hbm,
    ninput_hbm,
    nforget_hbm,
    wk_hbm,
    wv_hbm,
    keys_out,
    values_out,
    weight_out,
    score_out,
    base_out,
    floor_out,
    x_ref,
    gain_ref,
    wgate,
    conv_ref,
    shifts,
    fresh_rows,
    fresh_gates,
    wbuf,
    scaled,
    normed,
    rs,
    comp,
    gcomp,
    final,
    gfinal,
    ext,
    load_sem,
    send_sem,
    f_recv,
    ready,
):
    n, nsp, ns, nd, pos, heads, hl, dk, taps = dims
    G = 2
    length = nsp * pos
    width = x_ref.shape[2]
    nt = max(1, nd // ns)
    nq = max(1, ns // nd)
    t = lax.axis_index("tp")
    p = lax.axis_index("sp")
    low = 2 * t < n

    first = (p * nd) // ns
    late = n >= 4
    far = t == n - 1 if late else False
    barrier = pltpu.get_barrier_semaphore()

    def tell(semaphore, sp, tp):
        pl.semaphore_signal(
            semaphore, inc=1, device_id={"sp": sp, "tp": tp}, device_id_type=MESH
        )

    def greet(only_far):
        for m in range(nt):
            for a in range(nsp):
                to = first + m
                wanted = None if a else to != t
                if only_far:
                    wanted = to == n - 1 if a else (to == n - 1) & (to != t)

                def one(a=a, to=to):
                    tell(barrier, lax.rem(p + a, nsp), to)

                one() if wanted is None else pl.when(wanted)(one)

    own = ((t >= first) & (t < first + nt)).astype(jnp.int32)
    if late:

        @pl.when(far)
        def _():
            greet(True)

        @pl.when(jnp.logical_not(far))
        def _():
            for m in range(nq):
                tell(barrier, (t * ns) // nd + m, n - 1)
            greet(False)

        ends = ((first <= n - 1) & (n - 1 < first + nt)).astype(jnp.int32)
        expected = jnp.where(far, nq * n - own + nsp * (nt - ends), nq * (n - 1) - own)
    else:
        greet(False)
        expected = nq * n - own

    def answer():
        for m in range(nt):
            for a in range(nsp):

                @pl.when(first + m != n - 1)
                def _():
                    tell(ready, lax.rem(p + a, nsp), first + m)

    def target(k):
        down = jnp.where(k < n - 1 - t, n - 1 - k, n - 2 - k)
        if late:
            down = jnp.where(k == 0, n - 2, jnp.where(k == 1, n - 1, down))
        up = jnp.where(k < t, k, k + 1)
        return jnp.where(k == n - 1, t, jnp.where(low, down, up))

    def weight_copy(k, kv, head=0, count=hl, slot=2):
        columns = pl.ds(pl.multiple_of((target(k) * hl + head) * dk, dk), count * dk)
        source = wv_hbm if kv else wk_hbm
        place = wbuf.at[k, kv, :, head * dk : (head + count) * dk]
        return pltpu.make_async_copy(source.at[:, columns], place, load_sem.at[slot])

    early = pos // EARLY
    spans = ((0, early), (early, pos - early))
    x_copies = [
        pltpu.make_async_copy(
            x_hbm.at[:, lead : lead + rows], x_ref.at[:, lead : lead + rows], load_sem.at[at]
        )
        for at, (lead, rows) in enumerate(spans)
    ]
    gain_copy = pltpu.make_async_copy(gain_hbm, gain_ref, load_sem.at[2])
    key_first = weight_copy(0, 0, 0, 1, 3)
    key_rest = weight_copy(0, 0, 1, hl - 1, 4) if hl > 1 else None
    value_first = weight_copy(0, 1, 0, hl, 5)
    gain_copy.start()
    x_copies[0].start()
    key_first.start()
    x_copies[1].start()
    if key_rest is not None:
        key_rest.start()
    own_columns = pl.ds(pl.multiple_of(t * (hl * dk), dk), hl * dk)
    groups = (
        (wgate, ((wi_hbm, wgate.at[0:heads]), (wf_hbm, wgate.at[heads : 2 * heads]))),
        (conv_ref, ((conv_hbm.at[:, own_columns], conv_ref),)),
        (shifts, ((ishift_hbm, shifts.at[0]), (fshift_hbm, shifts.at[1]))),
        (
            fresh_rows,
            ((query_hbm, fresh_rows.at[0]), (nkey_hbm, fresh_rows.at[1]), (nvalue_hbm, fresh_rows.at[2])),
        ),
        (fresh_gates, ((ninput_hbm, fresh_gates.at[0]), (nforget_hbm, fresh_gates.at[1]))),
    )

    slots = (0, 1, 3, 4, 5)

    def load(g):
        for source, place in groups[g][1]:
            pltpu.make_async_copy(source, place, load_sem.at[slots[g]]).start()

    def loaded(g):
        whole = groups[g][0]
        pltpu.make_async_copy(whole, whole, load_sem.at[slots[g]]).wait()

    def start_rest():
        for k in range(1, n):
            for kv in range(2):
                weight_copy(k, kv).start()
        for g in range(1, len(groups)):
            load(g)

    gain_copy.wait()
    gain = gain_ref[...].astype(jnp.float32).reshape(1, -1)
    step = 32

    def scale(part):
        x_copies[part].wait()
        for i in range(ns):
            for at in range(spans[part][0], sum(spans[part]), step):
                wide = x_ref[i, at : at + step, :].astype(jnp.float32)
                scaled[i, at : at + step, :] = (wide * gain).astype(jnp.bfloat16)
                mean = jnp.mean(wide * wide, axis=-1, keepdims=True)
                rs[i, at : at + step, :] = jnp.broadcast_to(lax.rsqrt(mean + epsilon), (step, dk))

    def send(k, i, c, lead=0, rows=pos, head=0, count=hl):
        s = t * ns + i
        q = s // nd
        d = lax.rem(s, nd)
        to = k if c == G else target(k)
        mine = to == t
        if c == G:
            source, place = gcomp.at[k * ns + i], gfinal.at[d, p]
        else:
            source = comp.at[k * ns + i, c, head : head + count, lead : lead + rows, :]
            window = pl.ds(pl.multiple_of(p * pos + lead, rows & -rows), rows)
            place = (values_out if c else final).at[d, head : head + count, window, :]
        remote = pltpu.make_async_remote_copy(
            src_ref=source,
            dst_ref=place,
            send_sem=send_sem.at[c // G],
            recv_sem=f_recv.at[d, c],
            device_id={"sp": q, "tp": to},
            device_id_type=MESH,
        )
        away = jnp.logical_not(mine & (q == p))
        pl.when(away)(lambda: remote.start())

        @pl.when(jnp.logical_not(away))
        def _():
            pltpu.make_async_copy(source, place, f_recv.at[d, c]).start()

    def gates():
        loaded(0)
        for i in range(ns):

            @pl.loop(0, pos // step)
            def _(at):
                window = pl.ds(pl.multiple_of(at * step, step), step)
                wide = x_ref[i, window, :].astype(jnp.float32)
                normed[i, window, :] = (wide * rs[i, window, 0:1] * gain).astype(jnp.bfloat16)

            g = lax.dot_general(
                normed[i], wgate[...], (((1,), (1,)), ((), ())), preferred_element_type=jnp.float32
            )
            g = g.T
            for to in range(n):
                lines = [
                    g[base + to * hl + h : base + to * hl + h + 1, at * 128 : (at + 1) * 128]
                    for base in (0, heads)
                    for h in range(hl)
                    for at in range(pos // 128)
                ]
                gcomp[to * ns + i] = jnp.concatenate(lines, axis=0).astype(jnp.bfloat16)

    def project(k, kv, lead=0, rows=pos, head=0, count=hl):
        for i in range(ns):
            y = jnp.dot(
                scaled[i, lead : lead + rows],
                wbuf[k, kv, :, head * dk : (head + count) * dk],
                preferred_element_type=jnp.float32,
            )
            for h in range(count):
                comp[k * ns + i, kv, head + h, lead : lead + rows] = (
                    y[:, h * dk : (h + 1) * dk] * rs[i, lead : lead + rows]
                ).astype(jnp.bfloat16)

    def emit(k, kv, *piece):
        project(k, kv, *piece)
        if piece == (0, early, 0, 1):
            pl.semaphore_wait(barrier, expected)
        for i in range(ns):
            send(k, i, kv, *piece)

    scale(0)
    key_first.wait()
    value_first.start()
    load(0)
    emit(0, 0, 0, early, 0, 1)
    scale(1)
    emit(0, 0, early, pos - early, 0, 1)
    if late:
        pl.when(far)(answer)
    if key_rest is not None:
        key_rest.wait()
        emit(0, 0, 0, pos, 1, hl - 1)
    value_first.wait()
    start_rest()
    emit(0, 1)
    gates()
    if late:

        @pl.when(jnp.logical_not(far))
        def _():
            pl.semaphore_wait(ready, nq)

    for to in range(n):
        for i in range(ns):
            send(to, i, G)

    if n > 1:
        pltpu.make_async_copy(wbuf.at[1:n], wbuf.at[1:n], load_sem.at[2]).wait()

    @pl.loop(1, n)
    def _(k):
        for kv in range(2):
            emit(k, kv)

    def arrived(d, c):
        place = (final.at[d], values_out.at[d], gfinal.at[d])[c]
        pltpu.make_async_copy(place, place, f_recv.at[d, c]).wait()

    scaling = dk ** (-0.5)
    lane = lax.broadcasted_iota(jnp.int32, (8, length), 1)
    weights, fresh = {}, {}
    for g in range(1, len(groups)):
        loaded(g)

    for d in range(nd):
        arrived(d, G)
        for h in range(hl):

            def gate(which):
                lead = (which * hl + h) * (pos // 128)
                return jnp.concatenate(
                    [
                        gfinal[d, at].astype(jnp.float32)[lead + q : lead + q + 1]
                        for at in range(nsp)
                        for q in range(pos // 128)
                    ],
                    axis=1,
                )

            log_forget = log_sigmoid(gate(1) + shifts[1, d, h : h + 1, :])
            suffix = pltpu.roll(jnp.broadcast_to(log_forget, (8, length)), length - 1, 1)
            suffix = jnp.where(lane < length - 1, suffix, 0.0)
            hop = 1
            while hop < length:
                moved = pltpu.roll(suffix, length - hop, 1)
                suffix = suffix + jnp.where(lane < length - hop, moved, 0.0)
                hop *= 2
            new_input = fresh_gates[0, d : d + 1, h : h + 1]
            decay = log_sigmoid(fresh_gates[1, d : d + 1, h : h + 1])
            log_weight = gate(0) + shifts[0, d, h : h + 1, :] + suffix + decay
            largest = jnp.maximum(jnp.max(log_weight, axis=1, keepdims=True), new_input)
            weight = jnp.exp(log_weight - largest)
            weight_out[d, h : h + 1, :] = weight[0:1]
            query = fresh_rows[0, d, h : h + 1, :].astype(jnp.float32)
            match = jnp.sum(
                fresh_rows[1, d, h : h + 1, :].astype(jnp.float32) * query, axis=1, keepdims=True
            )
            score = jnp.exp(new_input - largest) * match * scaling
            fresh[d, h] = score.astype(jnp.bfloat16).astype(jnp.float32)
            weights[d, h] = weight

    for d in range(nd):
        ext[:, 0:8, :] = jnp.zeros((hl, 8, dk), jnp.float32)
        arrived(d, 0)
        for at in range(nsp):
            for h in range(hl):
                ext[h, 8 + at * pos : 8 + (at + 1) * pos, :] = final[
                    d, h, at * pos : (at + 1) * pos, :
                ].astype(jnp.float32)
                tap = conv_ref[:, h * dk : (h + 1) * dk]
                summed = None
                for o in range(taps):
                    start = 8 - (taps - 1) + o + at * pos
                    term = ext[h, start : start + pos, :] * tap[o : o + 1, :]
                    summed = term if summed is None else summed + term
                keys_out[d, h, at * pos : (at + 1) * pos, :] = jax.nn.silu(summed).astype(
                    jnp.bfloat16
                )
        for h in range(hl):
            query = jnp.broadcast_to(fresh_rows[0, d, h : h + 1, :], (8, dk))
            matched = lax.dot_general(
                query, keys_out[d, h], (((1,), (1,)), ((), ())), preferred_element_type=jnp.float32
            )
            score = (weights[d, h] * matched * scaling).astype(jnp.bfloat16)
            score_out[d, h] = score
            denominator = jnp.sum(score.astype(jnp.float32), axis=1, keepdims=True) + fresh[d, h]
            floor_out[d, h] = jnp.broadcast_to(jnp.maximum(jnp.abs(denominator), 1.0), (8, dk))
            base = fresh[d, h] * fresh_rows[2, d, h : h + 1, :].astype(jnp.float32)
            base_out[d, h] = jnp.broadcast_to(base, (8, dk))

    for d in range(nd):
        arrived(d, 1)

    kept = sum(((t * ns + i) // nd == p).astype(jnp.int32) for i in range(ns))
    for count in range(ns + 1):

        @pl.when(kept == count)
        def _():
            for c, buffer in enumerate((comp, gcomp)):
                place = buffer.at[0 : n * ns - count]
                pltpu.make_async_copy(place, place, send_sem.at[c]).wait()


def write_out(keys, values, weight, score, base, floor, keys_hbm, values_hbm, weight_hbm, read_hbm, read, sem):
    pairs = ((values, values_hbm), (keys, keys_hbm), (weight, weight_hbm), (read, read_hbm))
    copies = [pltpu.make_async_copy(*pair, sem.at[at]) for at, pair in enumerate(pairs)]
    for copy in copies[:3]:
        copy.start()
    nd, hl = values.shape[:2]
    for d in range(nd):
        for h in range(hl):
            numerator = jnp.dot(score[d, h], values[d, h], preferred_element_type=jnp.float32)
            result = (numerator + base[d, h]) / floor[d, h]
            read[d, h : h + 1, :] = result[0:1].astype(jnp.bfloat16)
    copies[3].start()
    for copy in copies:
        copy.wait()


def shards(
    n,
    nsp,
    layer_input,
    norm_gain,
    key_weight,
    value_weight,
    input_gate_weight,
    forget_gate_weight,
    conv_weight,
    input_shift,
    forget_shift,
    new_query,
    new_key,
    new_value,
    new_input,
    new_forget,
):
    ns, pos, width = layer_input.shape
    nd, hl, length = input_shift.shape
    dk = new_query.shape[2]
    heads = input_gate_weight.shape[1]
    taps = conv_weight.shape[0]
    dims = (n, nsp, ns, nd, pos, heads, hl, dk, taps)
    bf16, f32 = jnp.bfloat16, jnp.float32
    vmem = pl.BlockSpec(memory_space=pltpu.VMEM)
    hbm = pl.BlockSpec(memory_space=pltpu.HBM)
    dma = pltpu.SemaphoreType.DMA
    out_shape = (
        jax.ShapeDtypeStruct((nd, hl, length, dk), bf16),
        jax.ShapeDtypeStruct((nd, hl, length, dk), bf16),
        jax.ShapeDtypeStruct((nd, hl, length), f32),
        jax.ShapeDtypeStruct((nd, hl, dk), bf16),
    )
    held_shape = out_shape[:3] + (
        jax.ShapeDtypeStruct((nd, hl, 8, length), bf16),
        jax.ShapeDtypeStruct((nd, hl, 8, dk), f32),
        jax.ShapeDtypeStruct((nd, hl, 8, dk), f32),
    )
    held = pl.pallas_call(
        functools.partial(kernel, dims),
        out_shape=tuple(pltpu.VMEM(o.shape, o.dtype) for o in held_shape),
        in_specs=[hbm] * 14,
        out_specs=(vmem,) * 6,
        scratch_shapes=[
            pltpu.VMEM((ns, pos, width), bf16),
            pltpu.VMEM((width,), bf16),
            pltpu.VMEM((2 * heads, width), bf16),
            pltpu.VMEM((taps, hl * dk), f32),
            pltpu.VMEM((2, nd, hl, length), f32),
            pltpu.VMEM((3, nd, hl, dk), bf16),
            pltpu.VMEM((2, nd, hl), f32),
            pltpu.VMEM((n, 2, width, hl * dk), bf16),
            pltpu.VMEM((ns, pos, width), bf16),
            pltpu.VMEM((ns, pos, width), bf16),
            pltpu.VMEM((ns, pos, dk), f32),
            pltpu.VMEM((n * ns, 2, hl, pos, dk), bf16),
            pltpu.VMEM((n * ns, 2 * hl * pos // 128, 128), bf16),
            pltpu.VMEM((nd, hl, length, dk), bf16),
            pltpu.VMEM((nd, nsp, 2 * hl * pos // 128, 128), bf16),
            pltpu.VMEM((hl, 8 + length, dk), f32),
            dma((6,)),
            dma((2,)),
            dma((nd, 3)),
            pltpu.SemaphoreType.REGULAR,
        ],
        compiler_params=pltpu.CompilerParams(
            collective_id=0, has_side_effects=True, vmem_limit_bytes=60 * 1024 * 1024
        ),
    )(
        layer_input,
        norm_gain,
        input_gate_weight.T,
        forget_gate_weight.T,
        conv_weight,
        input_shift,
        forget_shift,
        new_query,
        new_key,
        new_value,
        new_input,
        new_forget,
        key_weight,
        value_weight,
    )
    return pl.pallas_call(
        write_out,
        out_shape=out_shape,
        in_specs=[vmem] * len(held_shape),
        out_specs=(hbm,) * len(out_shape),
        scratch_shapes=[pltpu.VMEM((nd, hl, dk), bf16), dma((len(out_shape),))],
        compiler_params=pltpu.CompilerParams(vmem_limit_bytes=8 * 1024 * 1024),
    )(*held)


def solution(mesh):
    in_specs = (
        P(("grp", "tp"), "sp", None),
        P(),
        P(),
        P(),
        P(),
        P(),
        P(),
        P(("grp", "sp"), "tp", None),
        P(("grp", "sp"), "tp", None),
        P(("grp", "sp"), "tp", None),
        P(("grp", "sp"), "tp", None),
        P(("grp", "sp"), "tp", None),
        P(("grp", "sp"), "tp"),
        P(("grp", "sp"), "tp"),
    )
    out_specs = (
        P(("grp", "sp"), "tp", None, None),
        P(("grp", "sp"), "tp", None, None),
        P(("grp", "sp"), "tp", None),
        P(("grp", "sp"), "tp", None),
    )
    body = functools.partial(shards, mesh.shape["tp"], mesh.shape["sp"])
    return jax.shard_map(body, mesh=mesh, in_specs=in_specs, out_specs=out_specs, check_vma=False)
```

```python
import functools

import jax
import jax.numpy as jnp
from jax import lax
from jax.experimental import pallas as pl
from jax.experimental.pallas import tpu as pltpu
from jax.sharding import PartitionSpec as P

MESH = pl.DeviceIdType.MESH
epsilon = 1e-06
EARLY = 2


def log_sigmoid(x):
    return jnp.minimum(x, 0.0) - jnp.log1p(jnp.exp(-jnp.abs(x)))


def kernel(
    dims,
    x_hbm,
    gain_hbm,
    wi_hbm,
    wf_hbm,
    conv_hbm,
    ishift_hbm,
    fshift_hbm,
    query_hbm,
    nkey_hbm,
    nvalue_hbm,
    ninput_hbm,
    nforget_hbm,
    wk_hbm,
    wv_hbm,
    keys_out,
    values_out,
    weight_out,
    score_out,
    base_out,
    floor_out,
    x_ref,
    gain_ref,
    wgate,
    conv_ref,
    shifts,
    fresh_rows,
    fresh_gates,
    wbuf,
    scaled,
    normed,
    rs,
    comp,
    gcomp,
    final,
    gfinal,
    ext,
    load_sem,
    send_sem,
    f_recv,
    ready,
):
    n, nsp, ns, nd, pos, heads, hl, dk, taps = dims
    G = 2
    length = nsp * pos
    width = x_ref.shape[2]
    nt = max(1, nd // ns)
    nq = max(1, ns // nd)
    t = lax.axis_index("tp")
    p = lax.axis_index("sp")
    low = 2 * t < n

    first = (p * nd) // ns
    late = n >= 4
    far = t == n - 1 if late else False
    barrier = pltpu.get_barrier_semaphore()

    def tell(semaphore, sp, tp):
        pl.semaphore_signal(
            semaphore, inc=1, device_id={"sp": sp, "tp": tp}, device_id_type=MESH
        )

    pair = 2 - nsp % 2
    lead = (p // pair) * pair
    peers = [lax.rem(lead + a, nsp) for a in range(pair, nsp)]
    peers += [lead + lax.rem(p + a, pair) for a in range(pair - 1, -1, -1)]

    def greet(only_far):
        for m in range(nt):
            for at, peer in enumerate(peers):
                a = nsp - 1 - at
                to = first + m
                wanted = None if a else to != t
                if only_far:
                    wanted = to == n - 1 if a else (to == n - 1) & (to != t)

                def one(peer=peer, to=to):
                    tell(barrier, peer, to)

                one() if wanted is None else pl.when(wanted)(one)

    own = ((t >= first) & (t < first + nt)).astype(jnp.int32)
    if late:

        @pl.when(far)
        def _():
            greet(True)

        @pl.when(jnp.logical_not(far))
        def _():
            greet(False)
            for m in range(nq):
                tell(barrier, (t * ns) // nd + m, n - 1)

        ends = ((first <= n - 1) & (n - 1 < first + nt)).astype(jnp.int32)
        expected = jnp.where(far, nq * n - own + nsp * (nt - ends), nq * (n - 1) - own)
    else:
        greet(False)
        expected = nq * n - own

    def answer():
        for m in range(nt):
            for a in range(nsp):

                @pl.when(first + m != n - 1)
                def _():
                    tell(ready, lax.rem(p + a, nsp), first + m)

    def target(k):
        down = jnp.where(k < n - 1 - t, n - 1 - k, n - 2 - k)
        if late:
            down = jnp.where(k == 0, n - 2, jnp.where(k == 1, n - 1, down))
        up = jnp.where(k < t, k, k + 1)
        return jnp.where(k == n - 1, t, jnp.where(low, down, up))

    def weight_copy(k, kv, head=0, count=hl, slot=2):
        columns = pl.ds(pl.multiple_of((target(k) * hl + head) * dk, dk), count * dk)
        source = wv_hbm if kv else wk_hbm
        place = wbuf.at[k, kv, :, head * dk : (head + count) * dk]
        return pltpu.make_async_copy(source.at[:, columns], place, load_sem.at[slot])

    early = pos // EARLY
    spans = ((0, early), (early, pos - early))
    x_copies = [
        pltpu.make_async_copy(
            x_hbm.at[:, lead : lead + rows], x_ref.at[:, lead : lead + rows], load_sem.at[at]
        )
        for at, (lead, rows) in enumerate(spans)
    ]
    gain_copy = pltpu.make_async_copy(gain_hbm, gain_ref, load_sem.at[2])
    key_first = weight_copy(0, 0, 0, 1, 3)
    key_rest = weight_copy(0, 0, 1, hl - 1, 4) if hl > 1 else None
    value_first = weight_copy(0, 1, 0, hl, 5)
    gain_copy.start()
    x_copies[0].start()
    key_first.start()
    x_copies[1].start()
    if key_rest is not None:
        key_rest.start()
    own_columns = pl.ds(pl.multiple_of(t * (hl * dk), dk), hl * dk)
    groups = (
        (wgate, ((wi_hbm, wgate.at[0:heads]), (wf_hbm, wgate.at[heads : 2 * heads]))),
        (conv_ref, ((conv_hbm.at[:, own_columns], conv_ref),)),
        (shifts, ((ishift_hbm, shifts.at[0]), (fshift_hbm, shifts.at[1]))),
        (
            fresh_rows,
            ((query_hbm, fresh_rows.at[0]), (nkey_hbm, fresh_rows.at[1]), (nvalue_hbm, fresh_rows.at[2])),
        ),
        (fresh_gates, ((ninput_hbm, fresh_gates.at[0]), (nforget_hbm, fresh_gates.at[1]))),
    )

    slots = (0, 1, 3, 4, 5)

    def load(g):
        for source, place in groups[g][1]:
            pltpu.make_async_copy(source, place, load_sem.at[slots[g]]).start()

    def loaded(g):
        whole = groups[g][0]
        pltpu.make_async_copy(whole, whole, load_sem.at[slots[g]]).wait()

    def start_rest():
        for k in range(1, n):
            for kv in range(2):
                weight_copy(k, kv).start()
        for g in range(1, len(groups)):
            load(g)

    gain_copy.wait()
    gain = gain_ref[...].astype(jnp.float32).reshape(1, -1)
    step = 32

    wide_gain = jnp.broadcast_to(gain, (16, width)).astype(jnp.bfloat16)

    def scale(part):
        lead, rows = spans[part]
        for i in range(ns):
            for at in range(lead, lead + rows, 16):
                scaled[i, at : at + 16, :] = x_ref[i, at : at + 16, :] * wide_gain
            for at in range(lead, lead + rows, step):
                wide = x_ref[i, at : at + step, :].astype(jnp.float32)
                mean = jnp.mean(wide * wide, axis=-1, keepdims=True)
                rs[i, at : at + step, :] = jnp.broadcast_to(lax.rsqrt(mean + epsilon), (step, dk))

    def send(k, i, c, lead=0, rows=pos, head=0, count=hl):
        s = t * ns + i
        q = s // nd
        d = lax.rem(s, nd)
        to = k if c == G else target(k)
        mine = to == t
        if c == G:
            source, place = gcomp.at[k * ns + i], gfinal.at[d, p]
        else:
            source = comp.at[k * ns + i, c, head : head + count, lead : lead + rows, :]
            window = pl.ds(pl.multiple_of(p * pos + lead, rows & -rows), rows)
            place = (values_out if c else final).at[d, head : head + count, window, :]
        remote = pltpu.make_async_remote_copy(
            src_ref=source,
            dst_ref=place,
            send_sem=send_sem.at[c // G],
            recv_sem=f_recv.at[d, c],
            device_id={"sp": q, "tp": to},
            device_id_type=MESH,
        )
        away = jnp.logical_not(mine & (q == p))
        pl.when(away)(lambda: remote.start())

        @pl.when(jnp.logical_not(away))
        def _():
            pltpu.make_async_copy(source, place, f_recv.at[d, c]).start()

    def gates():
        loaded(0)
        for i in range(ns):

            @pl.loop(0, pos // step)
            def _(at):
                window = pl.ds(pl.multiple_of(at * step, step), step)
                wide = x_ref[i, window, :].astype(jnp.float32)
                normed[i, window, :] = (wide * rs[i, window, 0:1] * gain).astype(jnp.bfloat16)

            g = lax.dot_general(
                normed[i], wgate[...], (((1,), (1,)), ((), ())), preferred_element_type=jnp.float32
            )
            g = g.T
            for to in range(n):
                lines = [
                    g[base + to * hl + h : base + to * hl + h + 1, at * 128 : (at + 1) * 128]
                    for base in (0, heads)
                    for h in range(hl)
                    for at in range(pos // 128)
                ]
                gcomp[to * ns + i] = jnp.concatenate(lines, axis=0).astype(jnp.bfloat16)

    def project(k, kv, lead=0, rows=pos, head=0, count=hl):
        opening = isinstance(k, int) and k == 0
        rounded = scaled if opening else normed
        for i in range(ns):
            y = jnp.dot(
                rounded[i, lead : lead + rows],
                wbuf[k, kv, :, head * dk : (head + count) * dk],
                preferred_element_type=jnp.float32,
            )
            for h in range(count):
                block = y[:, h * dk : (h + 1) * dk]
                if opening:
                    block = block * rs[i, lead : lead + rows]
                comp[k * ns + i, kv, head + h, lead : lead + rows] = block.astype(jnp.bfloat16)

    def emit(k, kv, *piece):
        project(k, kv, *piece)
        if piece == (0, early, 0, 1):
            pl.semaphore_wait(barrier, expected)
        for i in range(ns):
            send(k, i, kv, *piece)

    x_copies[0].wait()
    key_first.wait()
    value_first.start()
    load(0)
    scale(0)
    emit(0, 0, 0, early, 0, 1)
    x_copies[1].wait()
    scale(1)
    emit(0, 0, early, pos - early, 0, 1)
    if late:
        pl.when(far)(answer)
    if key_rest is not None:
        key_rest.wait()
        emit(0, 0, 0, pos, 1, hl - 1)
    value_first.wait()
    start_rest()
    emit(0, 1)
    gates()
    if late:

        @pl.when(jnp.logical_not(far))
        def _():
            pl.semaphore_wait(ready, nq)

    for to in range(n):
        for i in range(ns):
            send(to, i, G)

    if n > 1:
        pltpu.make_async_copy(wbuf.at[1:n], wbuf.at[1:n], load_sem.at[2]).wait()

    @pl.loop(1, n)
    def _(k):
        for kv in range(2):
            emit(k, kv)

    def arrived(d, c):
        place = (final.at[d], values_out.at[d], gfinal.at[d])[c]
        pltpu.make_async_copy(place, place, f_recv.at[d, c]).wait()

    scaling = dk ** (-0.5)
    lane = lax.broadcasted_iota(jnp.int32, (8, length), 1)
    weights, fresh = {}, {}
    for g in range(1, len(groups)):
        loaded(g)

    for d in range(nd):
        arrived(d, G)
        for h in range(hl):

            def gate(which):
                lead = (which * hl + h) * (pos // 128)
                return jnp.concatenate(
                    [
                        gfinal[d, at].astype(jnp.float32)[lead + q : lead + q + 1]
                        for at in range(nsp)
                        for q in range(pos // 128)
                    ],
                    axis=1,
                )

            log_forget = log_sigmoid(gate(1) + shifts[1, d, h : h + 1, :])
            suffix = pltpu.roll(jnp.broadcast_to(log_forget, (8, length)), length - 1, 1)
            suffix = jnp.where(lane < length - 1, suffix, 0.0)
            hop = 1
            while hop < length:
                moved = pltpu.roll(suffix, length - hop, 1)
                suffix = suffix + jnp.where(lane < length - hop, moved, 0.0)
                hop *= 2
            new_input = fresh_gates[0, d : d + 1, h : h + 1]
            decay = log_sigmoid(fresh_gates[1, d : d + 1, h : h + 1])
            log_weight = gate(0) + shifts[0, d, h : h + 1, :] + suffix + decay
            largest = jnp.maximum(jnp.max(log_weight, axis=1, keepdims=True), new_input)
            weight = jnp.exp(log_weight - largest)
            weight_out[d, h : h + 1, :] = weight[0:1]
            query = fresh_rows[0, d, h : h + 1, :].astype(jnp.float32)
            match = jnp.sum(
                fresh_rows[1, d, h : h + 1, :].astype(jnp.float32) * query, axis=1, keepdims=True
            )
            score = jnp.exp(new_input - largest) * match * scaling
            fresh[d, h] = score.astype(jnp.bfloat16).astype(jnp.float32)
            weights[d, h] = weight

    for d in range(nd):
        ext[:, 0:8, :] = jnp.zeros((hl, 8, dk), jnp.float32)
        arrived(d, 0)
        for at in range(nsp):
            for h in range(hl):
                ext[h, 8 + at * pos : 8 + (at + 1) * pos, :] = final[
                    d, h, at * pos : (at + 1) * pos, :
                ].astype(jnp.float32)
                tap = conv_ref[:, h * dk : (h + 1) * dk]
                summed = None
                for o in range(taps):
                    start = 8 - (taps - 1) + o + at * pos
                    term = ext[h, start : start + pos, :] * tap[o : o + 1, :]
                    summed = term if summed is None else summed + term
                keys_out[d, h, at * pos : (at + 1) * pos, :] = jax.nn.silu(summed).astype(
                    jnp.bfloat16
                )
        for h in range(hl):
            query = jnp.broadcast_to(fresh_rows[0, d, h : h + 1, :], (8, dk))
            matched = lax.dot_general(
                query, keys_out[d, h], (((1,), (1,)), ((), ())), preferred_element_type=jnp.float32
            )
            score = (weights[d, h] * matched * scaling).astype(jnp.bfloat16)
            score_out[d, h] = score
            denominator = jnp.sum(score.astype(jnp.float32), axis=1, keepdims=True) + fresh[d, h]
            floor_out[d, h] = jnp.broadcast_to(jnp.maximum(jnp.abs(denominator), 1.0), (8, dk))
            base = fresh[d, h] * fresh_rows[2, d, h : h + 1, :].astype(jnp.float32)
            base_out[d, h] = jnp.broadcast_to(base, (8, dk))

    kept = sum(((t * ns + i) // nd == p).astype(jnp.int32) for i in range(ns))
    for count in range(ns + 1):

        @pl.when(kept == count)
        def _():
            for c, buffer in enumerate((comp, gcomp)):
                place = buffer.at[0 : n * ns - count]
                pltpu.make_async_copy(place, place, send_sem.at[c]).wait()

    for d in range(nd):
        arrived(d, 1)


def write_out(keys, values, weight, score, base, floor, keys_hbm, values_hbm, weight_hbm, read_hbm, read, sem):
    pairs = ((values, values_hbm), (keys, keys_hbm), (weight, weight_hbm), (read, read_hbm))
    copies = [pltpu.make_async_copy(*pair, sem.at[at]) for at, pair in enumerate(pairs)]
    for copy in copies[:3]:
        copy.start()
    nd, hl = values.shape[:2]
    for d in range(nd):
        for h in range(hl):
            numerator = jnp.dot(score[d, h], values[d, h], preferred_element_type=jnp.float32)
            result = (numerator + base[d, h]) / floor[d, h]
            read[d, h : h + 1, :] = result[0:1].astype(jnp.bfloat16)
    copies[3].start()
    for copy in copies:
        copy.wait()


def shards(
    n,
    nsp,
    layer_input,
    norm_gain,
    key_weight,
    value_weight,
    input_gate_weight,
    forget_gate_weight,
    conv_weight,
    input_shift,
    forget_shift,
    new_query,
    new_key,
    new_value,
    new_input,
    new_forget,
):
    ns, pos, width = layer_input.shape
    nd, hl, length = input_shift.shape
    dk = new_query.shape[2]
    heads = input_gate_weight.shape[1]
    taps = conv_weight.shape[0]
    dims = (n, nsp, ns, nd, pos, heads, hl, dk, taps)
    bf16, f32 = jnp.bfloat16, jnp.float32
    vmem = pl.BlockSpec(memory_space=pltpu.VMEM)
    hbm = pl.BlockSpec(memory_space=pltpu.HBM)
    dma = pltpu.SemaphoreType.DMA
    out_shape = (
        jax.ShapeDtypeStruct((nd, hl, length, dk), bf16),
        jax.ShapeDtypeStruct((nd, hl, length, dk), bf16),
        jax.ShapeDtypeStruct((nd, hl, length), f32),
        jax.ShapeDtypeStruct((nd, hl, dk), bf16),
    )
    held_shape = out_shape[:3] + (
        jax.ShapeDtypeStruct((nd, hl, 8, length), bf16),
        jax.ShapeDtypeStruct((nd, hl, 8, dk), f32),
        jax.ShapeDtypeStruct((nd, hl, 8, dk), f32),
    )
    held = pl.pallas_call(
        functools.partial(kernel, dims),
        out_shape=tuple(pltpu.VMEM(o.shape, o.dtype) for o in held_shape),
        in_specs=[hbm] * 14,
        out_specs=(vmem,) * 6,
        scratch_shapes=[
            pltpu.VMEM((ns, pos, width), bf16),
            pltpu.VMEM((width,), bf16),
            pltpu.VMEM((2 * heads, width), bf16),
            pltpu.VMEM((taps, hl * dk), f32),
            pltpu.VMEM((2, nd, hl, length), f32),
            pltpu.VMEM((3, nd, hl, dk), bf16),
            pltpu.VMEM((2, nd, hl), f32),
            pltpu.VMEM((n, 2, width, hl * dk), bf16),
            pltpu.VMEM((ns, pos, width), bf16),
            pltpu.VMEM((ns, pos, width), bf16),
            pltpu.VMEM((ns, pos, dk), f32),
            pltpu.VMEM((n * ns, 2, hl, pos, dk), bf16),
            pltpu.VMEM((n * ns, 2 * hl * pos // 128, 128), bf16),
            pltpu.VMEM((nd, hl, length, dk), bf16),
            pltpu.VMEM((nd, nsp, 2 * hl * pos // 128, 128), bf16),
            pltpu.VMEM((hl, 8 + length, dk), f32),
            dma((6,)),
            dma((2,)),
            dma((nd, 3)),
            pltpu.SemaphoreType.REGULAR,
        ],
        compiler_params=pltpu.CompilerParams(
            collective_id=0, has_side_effects=True, vmem_limit_bytes=60 * 1024 * 1024
        ),
    )(
        layer_input,
        norm_gain,
        input_gate_weight.T,
        forget_gate_weight.T,
        conv_weight,
        input_shift,
        forget_shift,
        new_query,
        new_key,
        new_value,
        new_input,
        new_forget,
        key_weight,
        value_weight,
    )
    return pl.pallas_call(
        write_out,
        out_shape=out_shape,
        in_specs=[vmem] * len(held_shape),
        out_specs=(hbm,) * len(out_shape),
        scratch_shapes=[pltpu.VMEM((nd, hl, dk), bf16), dma((len(out_shape),))],
        compiler_params=pltpu.CompilerParams(vmem_limit_bytes=8 * 1024 * 1024),
    )(*held)


def solution(mesh):
    in_specs = (
        P(("grp", "tp"), "sp", None),
        P(),
        P(),
        P(),
        P(),
        P(),
        P(),
        P(("grp", "sp"), "tp", None),
        P(("grp", "sp"), "tp", None),
        P(("grp", "sp"), "tp", None),
        P(("grp", "sp"), "tp", None),
        P(("grp", "sp"), "tp", None),
        P(("grp", "sp"), "tp"),
        P(("grp", "sp"), "tp"),
    )
    out_specs = (
        P(("grp", "sp"), "tp", None, None),
        P(("grp", "sp"), "tp", None, None),
        P(("grp", "sp"), "tp", None),
        P(("grp", "sp"), "tp", None),
    )
    body = functools.partial(shards, mesh.shape["tp"], mesh.shape["sp"])
    return jax.shard_map(body, mesh=mesh, in_specs=in_specs, out_specs=out_specs, check_vma=False)
```

```python
import functools

import jax
import jax.numpy as jnp
from jax import lax
from jax.experimental import pallas as pl
from jax.experimental.pallas import tpu as pltpu
from jax.sharding import PartitionSpec as P

MESH = pl.DeviceIdType.MESH
epsilon = 1e-06
EARLY = 2


def log_sigmoid(x):
    return jnp.minimum(x, 0.0) - jnp.log1p(jnp.exp(-jnp.abs(x)))


def kernel(
    dims,
    x_hbm,
    gain_hbm,
    wi_hbm,
    wf_hbm,
    conv_hbm,
    ishift_hbm,
    fshift_hbm,
    query_hbm,
    nkey_hbm,
    nvalue_hbm,
    ninput_hbm,
    nforget_hbm,
    wk_hbm,
    wv_hbm,
    keys_out,
    values_out,
    weight_out,
    score_out,
    base_out,
    floor_out,
    x_ref,
    gain_ref,
    wgate,
    conv_ref,
    shifts,
    fresh_rows,
    fresh_gates,
    wbuf,
    scaled,
    normed,
    rs,
    comp,
    gcomp,
    final,
    gfinal,
    ext,
    load_sem,
    send_sem,
    f_recv,
    ready,
):
    n, nsp, ns, nd, pos, heads, hl, dk, taps = dims
    G = 2
    length = nsp * pos
    width = x_ref.shape[2]
    nt = max(1, nd // ns)
    nq = max(1, ns // nd)
    t = lax.axis_index("tp")
    p = lax.axis_index("sp")
    low = 2 * t < n

    first = (p * nd) // ns
    late = n >= 4
    far = t == n - 1 if late else False
    barrier = pltpu.get_barrier_semaphore()

    def tell(semaphore, sp, tp):
        pl.semaphore_signal(
            semaphore, inc=1, device_id={"sp": sp, "tp": tp}, device_id_type=MESH
        )

    pair = 2 - nsp % 2
    lead = (p // pair) * pair
    peers = [lax.rem(lead + a, nsp) for a in range(pair, nsp)]
    peers += [lead + lax.rem(p + a, pair) for a in range(pair - 1, -1, -1)]

    def greet(only_far):
        for m in range(nt):
            for at, peer in enumerate(peers):
                a = nsp - 1 - at
                to = first + m
                wanted = None if a else to != t
                if only_far:
                    wanted = to == n - 1 if a else (to == n - 1) & (to != t)

                def one(peer=peer, to=to):
                    tell(barrier, peer, to)

                one() if wanted is None else pl.when(wanted)(one)

    own = ((t >= first) & (t < first + nt)).astype(jnp.int32)
    if late:

        @pl.when(far)
        def _():
            greet(True)

        @pl.when(jnp.logical_not(far))
        def _():
            greet(False)
            for m in range(nq):
                tell(barrier, (t * ns) // nd + m, n - 1)

        ends = ((first <= n - 1) & (n - 1 < first + nt)).astype(jnp.int32)
        expected = jnp.where(far, nq * n - own + nsp * (nt - ends), nq * (n - 1) - own)
    else:
        greet(False)
        expected = nq * n - own

    def answer():
        for m in range(nt):
            for a in range(nsp):

                @pl.when(first + m != n - 1)
                def _():
                    tell(ready, lax.rem(p + a, nsp), first + m)

    def target(k):
        down = jnp.where(k < n - 1 - t, n - 1 - k, n - 2 - k)
        if late:
            down = jnp.where(k == 0, n - 2, jnp.where(k == 1, n - 1, down))
        up = jnp.where(k < t, k, k + 1)
        return jnp.where(k == n - 1, t, jnp.where(low, down, up))

    def weight_copy(k, kv, head=0, count=hl, slot=2):
        columns = pl.ds(pl.multiple_of((target(k) * hl + head) * dk, dk), count * dk)
        source = wv_hbm if kv else wk_hbm
        place = wbuf.at[k, kv, :, head * dk : (head + count) * dk]
        return pltpu.make_async_copy(source.at[:, columns], place, load_sem.at[slot])

    early = pos // EARLY
    spans = ((0, early), (early, pos - early))
    x_copies = [
        pltpu.make_async_copy(
            x_hbm.at[:, lead : lead + rows], x_ref.at[:, lead : lead + rows], load_sem.at[at]
        )
        for at, (lead, rows) in enumerate(spans)
    ]
    gain_copy = pltpu.make_async_copy(gain_hbm, gain_ref, load_sem.at[2])
    key_first = weight_copy(0, 0, 0, 1, 3)
    key_rest = weight_copy(0, 0, 1, hl - 1, 4) if hl > 1 else None
    value_first = weight_copy(0, 1, 0, hl, 5)
    gain_copy.start()
    x_copies[0].start()
    key_first.start()
    x_copies[1].start()
    if key_rest is not None:
        key_rest.start()
    own_columns = pl.ds(pl.multiple_of(t * (hl * dk), dk), hl * dk)
    groups = (
        (wgate, ((wi_hbm, wgate.at[0:heads]), (wf_hbm, wgate.at[heads : 2 * heads]))),
        (conv_ref, ((conv_hbm.at[:, own_columns], conv_ref),)),
        (shifts, ((ishift_hbm, shifts.at[0]), (fshift_hbm, shifts.at[1]))),
        (
            fresh_rows,
            ((query_hbm, fresh_rows.at[0]), (nkey_hbm, fresh_rows.at[1]), (nvalue_hbm, fresh_rows.at[2])),
        ),
        (fresh_gates, ((ninput_hbm, fresh_gates.at[0]), (nforget_hbm, fresh_gates.at[1]))),
    )

    slots = (0, 1, 3, 4, 5)

    def load(g):
        for source, place in groups[g][1]:
            pltpu.make_async_copy(source, place, load_sem.at[slots[g]]).start()

    def loaded(g):
        whole = groups[g][0]
        pltpu.make_async_copy(whole, whole, load_sem.at[slots[g]]).wait()

    def start_rest():
        for k in range(1, n):
            for kv in range(2):
                weight_copy(k, kv).start()
        for g in range(1, len(groups)):
            load(g)

    gain_copy.wait()
    gain = gain_ref[...].astype(jnp.float32).reshape(1, -1)
    step = 32

    wide_gain = jnp.broadcast_to(gain, (16, width)).astype(jnp.bfloat16)

    def scale(part):
        lead, rows = spans[part]
        for i in range(ns):
            for at in range(lead, lead + rows, 16):
                scaled[i, at : at + 16, :] = x_ref[i, at : at + 16, :] * wide_gain
            for at in range(lead, lead + rows, step):
                wide = x_ref[i, at : at + step, :].astype(jnp.float32)
                mean = jnp.mean(wide * wide, axis=-1, keepdims=True)
                rs[i, at : at + step, :] = jnp.broadcast_to(lax.rsqrt(mean + epsilon), (step, dk))

    def send(k, i, c, lead=0, rows=pos, head=0, count=hl):
        s = t * ns + i
        q = s // nd
        d = lax.rem(s, nd)
        to = k if c == G else target(k)
        mine = to == t
        if c == G:
            source, place = gcomp.at[k * ns + i], gfinal.at[d, p]
        else:
            source = comp.at[k * ns + i, c, head : head + count, lead : lead + rows, :]
            window = pl.ds(pl.multiple_of(p * pos + lead, rows & -rows), rows)
            place = (values_out if c else final).at[d, head : head + count, window, :]
        remote = pltpu.make_async_remote_copy(
            src_ref=source,
            dst_ref=place,
            send_sem=send_sem.at[c // G],
            recv_sem=f_recv.at[d, c],
            device_id={"sp": q, "tp": to},
            device_id_type=MESH,
        )
        away = jnp.logical_not(mine & (q == p))
        pl.when(away)(lambda: remote.start())

        @pl.when(jnp.logical_not(away))
        def _():
            pltpu.make_async_copy(source, place, f_recv.at[d, c]).start()

    def gates():
        loaded(0)
        for i in range(ns):

            @pl.loop(0, pos // step)
            def _(at):
                window = pl.ds(pl.multiple_of(at * step, step), step)
                wide = x_ref[i, window, :].astype(jnp.float32)
                normed[i, window, :] = (wide * rs[i, window, 0:1] * gain).astype(jnp.bfloat16)

            g = lax.dot_general(
                normed[i], wgate[...], (((1,), (1,)), ((), ())), preferred_element_type=jnp.float32
            )
            g = g.T
            for to in range(n):
                lines = [
                    g[base + to * hl + h : base + to * hl + h + 1, at * 128 : (at + 1) * 128]
                    for base in (0, heads)
                    for h in range(hl)
                    for at in range(pos // 128)
                ]
                gcomp[to * ns + i] = jnp.concatenate(lines, axis=0).astype(jnp.bfloat16)

    def project(k, kv, lead=0, rows=pos, head=0, count=hl):
        opening = isinstance(k, int) and k == 0
        rounded = scaled if opening else normed
        for i in range(ns):
            y = jnp.dot(
                rounded[i, lead : lead + rows],
                wbuf[k, kv, :, head * dk : (head + count) * dk],
                preferred_element_type=jnp.float32,
            )
            for h in range(count):
                block = y[:, h * dk : (h + 1) * dk]
                if opening:
                    block = block * rs[i, lead : lead + rows]
                comp[k * ns + i, kv, head + h, lead : lead + rows] = block.astype(jnp.bfloat16)

    def emit(k, kv, *piece):
        project(k, kv, *piece)
        if piece == (0, early, 0, 1):
            pl.semaphore_wait(barrier, expected)
        for i in range(ns):
            send(k, i, kv, *piece)

    x_copies[0].wait()
    key_first.wait()
    scale(0)
    emit(0, 0, 0, early, 0, 1)
    value_first.start()
    load(0)
    x_copies[1].wait()
    scale(1)
    emit(0, 0, early, pos - early, 0, 1)
    if late:
        pl.when(far)(answer)
    if key_rest is not None:
        key_rest.wait()
        emit(0, 0, 0, pos, 1, hl - 1)
    value_first.wait()
    start_rest()
    emit(0, 1)
    gates()
    if late:

        @pl.when(jnp.logical_not(far))
        def _():
            pl.semaphore_wait(ready, nq)

    for to in range(n):
        for i in range(ns):
            send(to, i, G)

    if n > 1:
        pltpu.make_async_copy(wbuf.at[1:n], wbuf.at[1:n], load_sem.at[2]).wait()

    @pl.loop(1, n)
    def _(k):
        for kv in range(2):
            emit(k, kv)

    def arrived(d, c):
        place = (final.at[d], values_out.at[d], gfinal.at[d])[c]
        pltpu.make_async_copy(place, place, f_recv.at[d, c]).wait()

    scaling = dk ** (-0.5)
    lane = lax.broadcasted_iota(jnp.int32, (8, length), 1)
    weights, fresh = {}, {}
    for g in range(1, len(groups)):
        loaded(g)

    for d in range(nd):
        arrived(d, G)
        for h in range(hl):

            def gate(which):
                lead = (which * hl + h) * (pos // 128)
                return jnp.concatenate(
                    [
                        gfinal[d, at].astype(jnp.float32)[lead + q : lead + q + 1]
                        for at in range(nsp)
                        for q in range(pos // 128)
                    ],
                    axis=1,
                )

            log_forget = log_sigmoid(gate(1) + shifts[1, d, h : h + 1, :])
            suffix = pltpu.roll(jnp.broadcast_to(log_forget, (8, length)), length - 1, 1)
            suffix = jnp.where(lane < length - 1, suffix, 0.0)
            hop = 1
            while hop < length:
                moved = pltpu.roll(suffix, length - hop, 1)
                suffix = suffix + jnp.where(lane < length - hop, moved, 0.0)
                hop *= 2
            new_input = fresh_gates[0, d : d + 1, h : h + 1]
            decay = log_sigmoid(fresh_gates[1, d : d + 1, h : h + 1])
            log_weight = gate(0) + shifts[0, d, h : h + 1, :] + suffix + decay
            largest = jnp.maximum(jnp.max(log_weight, axis=1, keepdims=True), new_input)
            weight = jnp.exp(log_weight - largest)
            weight_out[d, h : h + 1, :] = weight[0:1]
            query = fresh_rows[0, d, h : h + 1, :].astype(jnp.float32)
            match = jnp.sum(
                fresh_rows[1, d, h : h + 1, :].astype(jnp.float32) * query, axis=1, keepdims=True
            )
            score = jnp.exp(new_input - largest) * match * scaling
            fresh[d, h] = score.astype(jnp.bfloat16).astype(jnp.float32)
            weights[d, h] = weight

    for d in range(nd):
        ext[:, 0:8, :] = jnp.zeros((hl, 8, dk), jnp.float32)
        arrived(d, 0)
        for at in range(nsp):
            for h in range(hl):
                ext[h, 8 + at * pos : 8 + (at + 1) * pos, :] = final[
                    d, h, at * pos : (at + 1) * pos, :
                ].astype(jnp.float32)
                tap = conv_ref[:, h * dk : (h + 1) * dk]
                summed = None
                for o in range(taps):
                    start = 8 - (taps - 1) + o + at * pos
                    term = ext[h, start : start + pos, :] * tap[o : o + 1, :]
                    summed = term if summed is None else summed + term
                keys_out[d, h, at * pos : (at + 1) * pos, :] = jax.nn.silu(summed).astype(
                    jnp.bfloat16
                )
        for h in range(hl):
            query = jnp.broadcast_to(fresh_rows[0, d, h : h + 1, :], (8, dk))
            matched = lax.dot_general(
                query, keys_out[d, h], (((1,), (1,)), ((), ())), preferred_element_type=jnp.float32
            )
            score = (weights[d, h] * matched * scaling).astype(jnp.bfloat16)
            score_out[d, h] = score
            denominator = jnp.sum(score.astype(jnp.float32), axis=1, keepdims=True) + fresh[d, h]
            floor_out[d, h] = jnp.broadcast_to(jnp.maximum(jnp.abs(denominator), 1.0), (8, dk))
            base = fresh[d, h] * fresh_rows[2, d, h : h + 1, :].astype(jnp.float32)
            base_out[d, h] = jnp.broadcast_to(base, (8, dk))

    kept = sum(((t * ns + i) // nd == p).astype(jnp.int32) for i in range(ns))
    for count in range(ns + 1):

        @pl.when(kept == count)
        def _():
            for c, buffer in enumerate((comp, gcomp)):
                place = buffer.at[0 : n * ns - count]
                pltpu.make_async_copy(place, place, send_sem.at[c]).wait()

    for d in range(nd):
        arrived(d, 1)


def write_out(keys, values, weight, score, base, floor, keys_hbm, values_hbm, weight_hbm, read_hbm, read, sem):
    pairs = ((values, values_hbm), (keys, keys_hbm), (weight, weight_hbm), (read, read_hbm))
    copies = [pltpu.make_async_copy(*pair, sem.at[at]) for at, pair in enumerate(pairs)]
    for copy in copies[:3]:
        copy.start()
    nd, hl = values.shape[:2]
    for d in range(nd):
        for h in range(hl):
            numerator = jnp.dot(score[d, h], values[d, h], preferred_element_type=jnp.float32)
            result = (numerator + base[d, h]) / floor[d, h]
            read[d, h : h + 1, :] = result[0:1].astype(jnp.bfloat16)
    copies[3].start()
    for copy in copies:
        copy.wait()


def shards(
    n,
    nsp,
    layer_input,
    norm_gain,
    key_weight,
    value_weight,
    input_gate_weight,
    forget_gate_weight,
    conv_weight,
    input_shift,
    forget_shift,
    new_query,
    new_key,
    new_value,
    new_input,
    new_forget,
):
    ns, pos, width = layer_input.shape
    nd, hl, length = input_shift.shape
    dk = new_query.shape[2]
    heads = input_gate_weight.shape[1]
    taps = conv_weight.shape[0]
    dims = (n, nsp, ns, nd, pos, heads, hl, dk, taps)
    bf16, f32 = jnp.bfloat16, jnp.float32
    vmem = pl.BlockSpec(memory_space=pltpu.VMEM)
    hbm = pl.BlockSpec(memory_space=pltpu.HBM)
    dma = pltpu.SemaphoreType.DMA
    out_shape = (
        jax.ShapeDtypeStruct((nd, hl, length, dk), bf16),
        jax.ShapeDtypeStruct((nd, hl, length, dk), bf16),
        jax.ShapeDtypeStruct((nd, hl, length), f32),
        jax.ShapeDtypeStruct((nd, hl, dk), bf16),
    )
    held_shape = out_shape[:3] + (
        jax.ShapeDtypeStruct((nd, hl, 8, length), bf16),
        jax.ShapeDtypeStruct((nd, hl, 8, dk), f32),
        jax.ShapeDtypeStruct((nd, hl, 8, dk), f32),
    )
    held = pl.pallas_call(
        functools.partial(kernel, dims),
        out_shape=tuple(pltpu.VMEM(o.shape, o.dtype) for o in held_shape),
        in_specs=[hbm] * 14,
        out_specs=(vmem,) * 6,
        scratch_shapes=[
            pltpu.VMEM((ns, pos, width), bf16),
            pltpu.VMEM((width,), bf16),
            pltpu.VMEM((2 * heads, width), bf16),
            pltpu.VMEM((taps, hl * dk), f32),
            pltpu.VMEM((2, nd, hl, length), f32),
            pltpu.VMEM((3, nd, hl, dk), bf16),
            pltpu.VMEM((2, nd, hl), f32),
            pltpu.VMEM((n, 2, width, hl * dk), bf16),
            pltpu.VMEM((ns, pos, width), bf16),
            pltpu.VMEM((ns, pos, width), bf16),
            pltpu.VMEM((ns, pos, dk), f32),
            pltpu.VMEM((n * ns, 2, hl, pos, dk), bf16),
            pltpu.VMEM((n * ns, 2 * hl * pos // 128, 128), bf16),
            pltpu.VMEM((nd, hl, length, dk), bf16),
            pltpu.VMEM((nd, nsp, 2 * hl * pos // 128, 128), bf16),
            pltpu.VMEM((hl, 8 + length, dk), f32),
            dma((6,)),
            dma((2,)),
            dma((nd, 3)),
            pltpu.SemaphoreType.REGULAR,
        ],
        compiler_params=pltpu.CompilerParams(
            collective_id=0, has_side_effects=True, vmem_limit_bytes=60 * 1024 * 1024
        ),
    )(
        layer_input,
        norm_gain,
        input_gate_weight.T,
        forget_gate_weight.T,
        conv_weight,
        input_shift,
        forget_shift,
        new_query,
        new_key,
        new_value,
        new_input,
        new_forget,
        key_weight,
        value_weight,
    )
    return pl.pallas_call(
        write_out,
        out_shape=out_shape,
        in_specs=[vmem] * len(held_shape),
        out_specs=(hbm,) * len(out_shape),
        scratch_shapes=[pltpu.VMEM((nd, hl, dk), bf16), dma((len(out_shape),))],
        compiler_params=pltpu.CompilerParams(vmem_limit_bytes=8 * 1024 * 1024),
    )(*held)


def solution(mesh):
    in_specs = (
        P(("grp", "tp"), "sp", None),
        P(),
        P(),
        P(),
        P(),
        P(),
        P(),
        P(("grp", "sp"), "tp", None),
        P(("grp", "sp"), "tp", None),
        P(("grp", "sp"), "tp", None),
        P(("grp", "sp"), "tp", None),
        P(("grp", "sp"), "tp", None),
        P(("grp", "sp"), "tp"),
        P(("grp", "sp"), "tp"),
    )
    out_specs = (
        P(("grp", "sp"), "tp", None, None),
        P(("grp", "sp"), "tp", None, None),
        P(("grp", "sp"), "tp", None),
        P(("grp", "sp"), "tp", None),
    )
    body = functools.partial(shards, mesh.shape["tp"], mesh.shape["sp"])
    return jax.shard_map(body, mesh=mesh, in_specs=in_specs, out_specs=out_specs, check_vma=False)
```

```python
import functools

import jax
import jax.numpy as jnp
from jax import lax
from jax.experimental import pallas as pl
from jax.experimental.pallas import tpu as pltpu
from jax.sharding import PartitionSpec as P

MESH = pl.DeviceIdType.MESH
epsilon = 1e-06
EARLY = 2


def log_sigmoid(x):
    return jnp.minimum(x, 0.0) - jnp.log1p(jnp.exp(-jnp.abs(x)))


def kernel(
    dims,
    x_hbm,
    gain_hbm,
    wi_hbm,
    wf_hbm,
    conv_hbm,
    ishift_hbm,
    fshift_hbm,
    query_hbm,
    nkey_hbm,
    nvalue_hbm,
    ninput_hbm,
    nforget_hbm,
    wk_hbm,
    wv_hbm,
    keys_out,
    values_out,
    weight_out,
    score_out,
    base_out,
    floor_out,
    x_ref,
    gain_ref,
    wgate,
    conv_ref,
    shifts,
    fresh_rows,
    fresh_gates,
    wbuf,
    scaled,
    normed,
    rs,
    comp,
    gcomp,
    final,
    gfinal,
    ext,
    load_sem,
    send_sem,
    f_recv,
    ready,
):
    n, nsp, ns, nd, pos, heads, hl, dk, taps = dims
    G = 2
    length = nsp * pos
    width = x_ref.shape[2]
    nt = max(1, nd // ns)
    nq = max(1, ns // nd)
    t = lax.axis_index("tp")
    p = lax.axis_index("sp")
    low = 2 * t < n

    first = (p * nd) // ns
    late = n >= 4
    far = t == n - 1 if late else False
    barrier = pltpu.get_barrier_semaphore()

    def tell(semaphore, sp, tp):
        pl.semaphore_signal(
            semaphore, inc=1, device_id={"sp": sp, "tp": tp}, device_id_type=MESH
        )

    pair = 2 - nsp % 2
    lead = (p // pair) * pair
    peers = [lax.rem(lead + a, nsp) for a in range(pair, nsp)]
    peers += [lead + lax.rem(p + a, pair) for a in range(pair - 1, -1, -1)]

    def greet(only_far):
        for m in range(nt):
            for at, peer in enumerate(peers):
                a = nsp - 1 - at
                to = first + m
                wanted = None if a else to != t
                if only_far:
                    wanted = to == n - 1 if a else (to == n - 1) & (to != t)

                def one(peer=peer, to=to):
                    tell(barrier, peer, to)

                one() if wanted is None else pl.when(wanted)(one)

    own = ((t >= first) & (t < first + nt)).astype(jnp.int32)
    if late:

        @pl.when(far)
        def _():
            greet(True)

        @pl.when(jnp.logical_not(far))
        def _():
            greet(False)
            for m in range(nq):
                tell(barrier, (t * ns) // nd + m, n - 1)

        ends = ((first <= n - 1) & (n - 1 < first + nt)).astype(jnp.int32)
        expected = jnp.where(far, nq * n - own + nsp * (nt - ends), nq * (n - 1) - own)
    else:
        greet(False)
        expected = nq * n - own

    def answer():
        for m in range(nt):
            for a in range(nsp):

                @pl.when(first + m != n - 1)
                def _():
                    tell(ready, lax.rem(p + a, nsp), first + m)

    def target(k):
        down = jnp.where(k < n - 1 - t, n - 1 - k, n - 2 - k)
        if late:
            down = jnp.where(k == 0, n - 2, jnp.where(k == 1, n - 1, down))
        up = jnp.where(k < t, k, k + 1)
        return jnp.where(k == n - 1, t, jnp.where(low, down, up))

    def weight_copy(k, kv, head=0, count=hl, slot=2):
        columns = pl.ds(pl.multiple_of((target(k) * hl + head) * dk, dk), count * dk)
        source = wv_hbm if kv else wk_hbm
        place = wbuf.at[k, kv, :, head * dk : (head + count) * dk]
        return pltpu.make_async_copy(source.at[:, columns], place, load_sem.at[slot])

    early = pos // EARLY
    spans = ((0, early), (early, pos - early))
    x_copies = [
        pltpu.make_async_copy(
            x_hbm.at[:, lead : lead + rows], x_ref.at[:, lead : lead + rows], load_sem.at[at]
        )
        for at, (lead, rows) in enumerate(spans)
    ]
    gain_copy = pltpu.make_async_copy(gain_hbm, gain_ref, load_sem.at[2])
    key_first = weight_copy(0, 0, 0, 1, 3)
    key_rest = weight_copy(0, 0, 1, hl - 1, 4) if hl > 1 else None
    value_first = weight_copy(0, 1, 0, hl, 5)
    gain_copy.start()
    x_copies[0].start()
    key_first.start()
    x_copies[1].start()
    if key_rest is not None:
        key_rest.start()
    own_columns = pl.ds(pl.multiple_of(t * (hl * dk), dk), hl * dk)
    groups = (
        (wgate, ((wi_hbm, wgate.at[0:heads]), (wf_hbm, wgate.at[heads : 2 * heads]))),
        (conv_ref, ((conv_hbm.at[:, own_columns], conv_ref),)),
        (shifts, ((ishift_hbm, shifts.at[0]), (fshift_hbm, shifts.at[1]))),
        (
            fresh_rows,
            ((query_hbm, fresh_rows.at[0]), (nkey_hbm, fresh_rows.at[1]), (nvalue_hbm, fresh_rows.at[2])),
        ),
        (fresh_gates, ((ninput_hbm, fresh_gates.at[0]), (nforget_hbm, fresh_gates.at[1]))),
    )

    slots = (0, 1, 3, 4, 5)

    def load(g):
        for source, place in groups[g][1]:
            pltpu.make_async_copy(source, place, load_sem.at[slots[g]]).start()

    def loaded(g):
        whole = groups[g][0]
        pltpu.make_async_copy(whole, whole, load_sem.at[slots[g]]).wait()

    def start_rest():
        for k in range(1, n):
            for kv in range(2):
                weight_copy(k, kv).start()
        for g in range(1, len(groups)):
            load(g)

    gain_copy.wait()
    gain = gain_ref[...].astype(jnp.float32).reshape(1, -1)
    step = 32

    wide_gain = jnp.broadcast_to(gain, (16, width)).astype(jnp.bfloat16)

    def scale(part):
        lead, rows = spans[part]
        for i in range(ns):
            for at in range(lead, lead + rows, 16):
                scaled[i, at : at + 16, :] = x_ref[i, at : at + 16, :] * wide_gain
            for at in range(lead, lead + rows, step):
                wide = x_ref[i, at : at + step, :].astype(jnp.float32)
                mean = jnp.mean(wide * wide, axis=-1, keepdims=True)
                rs[i, at : at + step, :] = jnp.broadcast_to(lax.rsqrt(mean + epsilon), (step, dk))

    def send(k, i, c, lead=0, rows=pos, head=0, count=hl):
        s = t * ns + i
        q = s // nd
        d = lax.rem(s, nd)
        to = k if c == G else target(k)
        mine = to == t
        if c == G:
            source, place = gcomp.at[k * ns + i], gfinal.at[d, p]
        else:
            source = comp.at[k * ns + i, c, head : head + count, lead : lead + rows, :]
            window = pl.ds(pl.multiple_of(p * pos + lead, rows & -rows), rows)
            place = (values_out if c else final).at[d, head : head + count, window, :]
        remote = pltpu.make_async_remote_copy(
            src_ref=source,
            dst_ref=place,
            send_sem=send_sem.at[c // G],
            recv_sem=f_recv.at[d, c],
            device_id={"sp": q, "tp": to},
            device_id_type=MESH,
        )
        away = jnp.logical_not(mine & (q == p))
        pl.when(away)(lambda: remote.start())

        @pl.when(jnp.logical_not(away))
        def _():
            pltpu.make_async_copy(source, place, f_recv.at[d, c]).start()

    def gates():
        loaded(0)
        for i in range(ns):

            @pl.loop(0, pos // step)
            def _(at):
                window = pl.ds(pl.multiple_of(at * step, step), step)
                wide = x_ref[i, window, :].astype(jnp.float32)
                normed[i, window, :] = (wide * rs[i, window, 0:1] * gain).astype(jnp.bfloat16)

            g = lax.dot_general(
                normed[i], wgate[...], (((1,), (1,)), ((), ())), preferred_element_type=jnp.float32
            )
            g = g.T
            for to in range(n):
                lines = [
                    g[base + to * hl + h : base + to * hl + h + 1, at * 128 : (at + 1) * 128]
                    for base in (0, heads)
                    for h in range(hl)
                    for at in range(pos // 128)
                ]
                gcomp[to * ns + i] = jnp.concatenate(lines, axis=0).astype(jnp.bfloat16)

    def project(k, kv, lead=0, rows=pos, head=0, count=hl):
        opening = isinstance(k, int) and k == 0
        rounded = scaled if opening else normed
        for i in range(ns):
            y = jnp.dot(
                rounded[i, lead : lead + rows],
                wbuf[k, kv, :, head * dk : (head + count) * dk],
                preferred_element_type=jnp.float32,
            )
            for h in range(count):
                block = y[:, h * dk : (h + 1) * dk]
                if opening:
                    block = block * rs[i, lead : lead + rows]
                comp[k * ns + i, kv, head + h, lead : lead + rows] = block.astype(jnp.bfloat16)

    def emit(k, kv, *piece):
        project(k, kv, *piece)
        if piece == (0, early, 0, 1):
            pl.semaphore_wait(barrier, expected)
        for i in range(ns):
            send(k, i, kv, *piece)

    x_copies[0].wait()
    key_first.wait()
    scale(0)
    emit(0, 0, 0, early, 0, 1)
    value_first.start()
    load(0)
    x_copies[1].wait()
    scale(1)
    emit(0, 0, early, pos - early, 0, 1)
    if late:
        pl.when(far)(answer)
    if key_rest is not None:
        key_rest.wait()
        emit(0, 0, 0, pos, 1, hl - 1)
    value_first.wait()
    start_rest()
    emit(0, 1)
    gates()
    if late:

        @pl.when(jnp.logical_not(far))
        def _():
            pl.semaphore_wait(ready, nq)

    for to in range(n):
        for i in range(ns):
            send(to, i, G)

    if n > 1:
        pltpu.make_async_copy(wbuf.at[1:n], wbuf.at[1:n], load_sem.at[2]).wait()

    @pl.loop(1, n)
    def _(k):
        for kv in range(2):
            emit(k, kv)

    def arrived(d, c):
        place = (final.at[d], values_out.at[d], gfinal.at[d])[c]
        pltpu.make_async_copy(place, place, f_recv.at[d, c]).wait()

    scaling = dk ** (-0.5)
    lane = lax.broadcasted_iota(jnp.int32, (8, length), 1)
    weights, fresh = {}, {}
    for g in range(1, len(groups)):
        loaded(g)

    for d in range(nd):
        arrived(d, G)
        for h in range(hl):

            def gate(which):
                lead = (which * hl + h) * (pos // 128)
                return jnp.concatenate(
                    [
                        gfinal[d, at].astype(jnp.float32)[lead + q : lead + q + 1]
                        for at in range(nsp)
                        for q in range(pos // 128)
                    ],
                    axis=1,
                )

            log_forget = log_sigmoid(gate(1) + shifts[1, d, h : h + 1, :])
            suffix = pltpu.roll(jnp.broadcast_to(log_forget, (8, length)), length - 1, 1)
            suffix = jnp.where(lane < length - 1, suffix, 0.0)
            hop = 1
            while hop < length:
                moved = pltpu.roll(suffix, length - hop, 1)
                suffix = suffix + jnp.where(lane < length - hop, moved, 0.0)
                hop *= 2
            new_input = fresh_gates[0, d : d + 1, h : h + 1]
            decay = log_sigmoid(fresh_gates[1, d : d + 1, h : h + 1])
            log_weight = gate(0) + shifts[0, d, h : h + 1, :] + suffix + decay
            largest = jnp.maximum(jnp.max(log_weight, axis=1, keepdims=True), new_input)
            weight = jnp.exp(log_weight - largest)
            weight_out[d, h : h + 1, :] = weight[0:1]
            query = fresh_rows[0, d, h : h + 1, :].astype(jnp.float32)
            match = jnp.sum(
                fresh_rows[1, d, h : h + 1, :].astype(jnp.float32) * query, axis=1, keepdims=True
            )
            score = jnp.exp(new_input - largest) * match * scaling
            fresh[d, h] = score.astype(jnp.bfloat16).astype(jnp.float32)
            weights[d, h] = weight

    for d in range(nd):
        ext[:, 0:8, :] = jnp.zeros((hl, 8, dk), jnp.float32)
        arrived(d, 0)
        for at in range(nsp):
            for h in range(hl):
                ext[h, 8 + at * pos : 8 + (at + 1) * pos, :] = final[
                    d, h, at * pos : (at + 1) * pos, :
                ].astype(jnp.float32)
                tap = conv_ref[:, h * dk : (h + 1) * dk]
                summed = None
                for o in range(taps):
                    start = 8 - (taps - 1) + o + at * pos
                    term = ext[h, start : start + pos, :] * tap[o : o + 1, :]
                    summed = term if summed is None else summed + term
                keys_out[d, h, at * pos : (at + 1) * pos, :] = jax.nn.silu(summed).astype(
                    jnp.bfloat16
                )
        for h in range(hl):
            query = jnp.broadcast_to(fresh_rows[0, d, h : h + 1, :], (8, dk))
            matched = lax.dot_general(
                query, keys_out[d, h], (((1,), (1,)), ((), ())), preferred_element_type=jnp.float32
            )
            score = (weights[d, h] * matched * scaling).astype(jnp.bfloat16)
            score_out[d, h] = score
            denominator = jnp.sum(score.astype(jnp.float32), axis=1, keepdims=True) + fresh[d, h]
            floor_out[d, h] = jnp.broadcast_to(jnp.maximum(jnp.abs(denominator), 1.0), (8, dk))
            base = fresh[d, h] * fresh_rows[2, d, h : h + 1, :].astype(jnp.float32)
            base_out[d, h] = jnp.broadcast_to(base, (8, dk))

    kept = sum(((t * ns + i) // nd == p).astype(jnp.int32) for i in range(ns))
    for count in range(ns + 1):

        @pl.when(kept == count)
        def _():
            for c, buffer in enumerate((comp, gcomp)):
                place = buffer.at[0 : n * ns - count]
                pltpu.make_async_copy(place, place, send_sem.at[c]).wait()

    for d in range(nd):
        arrived(d, 1)


def write_out(keys, values, weight, score, base, floor, keys_hbm, values_hbm, weight_hbm, read_hbm, read, sem):
    pairs = ((weight, weight_hbm), (keys, keys_hbm), (values, values_hbm), (read, read_hbm))
    copies = [pltpu.make_async_copy(*pair, sem.at[at]) for at, pair in enumerate(pairs)]
    for copy in copies[:3]:
        copy.start()
    nd, hl = values.shape[:2]
    for d in range(nd):
        for h in range(hl):
            numerator = jnp.dot(score[d, h], values[d, h], preferred_element_type=jnp.float32)
            result = (numerator + base[d, h]) / floor[d, h]
            read[d, h : h + 1, :] = result[0:1].astype(jnp.bfloat16)
    copies[3].start()
    for copy in copies:
        copy.wait()


def shards(
    n,
    nsp,
    layer_input,
    norm_gain,
    key_weight,
    value_weight,
    input_gate_weight,
    forget_gate_weight,
    conv_weight,
    input_shift,
    forget_shift,
    new_query,
    new_key,
    new_value,
    new_input,
    new_forget,
):
    ns, pos, width = layer_input.shape
    nd, hl, length = input_shift.shape
    dk = new_query.shape[2]
    heads = input_gate_weight.shape[1]
    taps = conv_weight.shape[0]
    dims = (n, nsp, ns, nd, pos, heads, hl, dk, taps)
    bf16, f32 = jnp.bfloat16, jnp.float32
    vmem = pl.BlockSpec(memory_space=pltpu.VMEM)
    hbm = pl.BlockSpec(memory_space=pltpu.HBM)
    dma = pltpu.SemaphoreType.DMA
    out_shape = (
        jax.ShapeDtypeStruct((nd, hl, length, dk), bf16),
        jax.ShapeDtypeStruct((nd, hl, length, dk), bf16),
        jax.ShapeDtypeStruct((nd, hl, length), f32),
        jax.ShapeDtypeStruct((nd, hl, dk), bf16),
    )
    held_shape = out_shape[:3] + (
        jax.ShapeDtypeStruct((nd, hl, 8, length), bf16),
        jax.ShapeDtypeStruct((nd, hl, 8, dk), f32),
        jax.ShapeDtypeStruct((nd, hl, 8, dk), f32),
    )
    held = pl.pallas_call(
        functools.partial(kernel, dims),
        out_shape=tuple(pltpu.VMEM(o.shape, o.dtype) for o in held_shape),
        in_specs=[hbm] * 14,
        out_specs=(vmem,) * 6,
        scratch_shapes=[
            pltpu.VMEM((ns, pos, width), bf16),
            pltpu.VMEM((width,), bf16),
            pltpu.VMEM((2 * heads, width), bf16),
            pltpu.VMEM((taps, hl * dk), f32),
            pltpu.VMEM((2, nd, hl, length), f32),
            pltpu.VMEM((3, nd, hl, dk), bf16),
            pltpu.VMEM((2, nd, hl), f32),
            pltpu.VMEM((n, 2, width, hl * dk), bf16),
            pltpu.VMEM((ns, pos, width), bf16),
            pltpu.VMEM((ns, pos, width), bf16),
            pltpu.VMEM((ns, pos, dk), f32),
            pltpu.VMEM((n * ns, 2, hl, pos, dk), bf16),
            pltpu.VMEM((n * ns, 2 * hl * pos // 128, 128), bf16),
            pltpu.VMEM((nd, hl, length, dk), bf16),
            pltpu.VMEM((nd, nsp, 2 * hl * pos // 128, 128), bf16),
            pltpu.VMEM((hl, 8 + length, dk), f32),
            dma((6,)),
            dma((2,)),
            dma((nd, 3)),
            pltpu.SemaphoreType.REGULAR,
        ],
        compiler_params=pltpu.CompilerParams(
            collective_id=0, has_side_effects=True, vmem_limit_bytes=60 * 1024 * 1024
        ),
    )(
        layer_input,
        norm_gain,
        input_gate_weight.T,
        forget_gate_weight.T,
        conv_weight,
        input_shift,
        forget_shift,
        new_query,
        new_key,
        new_value,
        new_input,
        new_forget,
        key_weight,
        value_weight,
    )
    return pl.pallas_call(
        write_out,
        out_shape=out_shape,
        in_specs=[vmem] * len(held_shape),
        out_specs=(hbm,) * len(out_shape),
        scratch_shapes=[pltpu.VMEM((nd, hl, dk), bf16), dma((len(out_shape),))],
        compiler_params=pltpu.CompilerParams(vmem_limit_bytes=8 * 1024 * 1024),
    )(*held)


def solution(mesh):
    in_specs = (
        P(("grp", "tp"), "sp", None),
        P(),
        P(),
        P(),
        P(),
        P(),
        P(),
        P(("grp", "sp"), "tp", None),
        P(("grp", "sp"), "tp", None),
        P(("grp", "sp"), "tp", None),
        P(("grp", "sp"), "tp", None),
        P(("grp", "sp"), "tp", None),
        P(("grp", "sp"), "tp"),
        P(("grp", "sp"), "tp"),
    )
    out_specs = (
        P(("grp", "sp"), "tp", None, None),
        P(("grp", "sp"), "tp", None, None),
        P(("grp", "sp"), "tp", None),
        P(("grp", "sp"), "tp", None),
    )
    body = functools.partial(shards, mesh.shape["tp"], mesh.shape["sp"])
    return jax.shard_map(body, mesh=mesh, in_specs=in_specs, out_specs=out_specs, check_vma=False)
```
